512 devices in a mesh: sp: 16 (over z), fs: 4 (over y), tp: 8 (over x, core).
Axes of the slice: x: 4, y: 4, z: 16, core: 2. Of those that a mesh axis runs over, the one named last changes fastest.
Arguments:
- tokens: bfloat16 [32768, 2048], P(('fs', 'sp')), parts along dimension 0, may hold values from -6 to 6
- norm_gain: float32 [2048], replicated, may hold values from 0.1 to 1.9
- state_gate: bfloat16 [2048, 1024], P('sp', 'tp'), may hold values from -0.125 to 0.125
- state_value: bfloat16 [2048, 1024], P('sp', 'tp'), may hold values from -0.125 to 0.125
- state_keys: bfloat16 [2048, 1024], P('sp', 'tp'), may hold values from -0.125 to 0.125
- state_query: bfloat16 [2048, 1024], P('sp', 'tp'), may hold values from -0.125 to 0.125
- state_step: bfloat16 [2048, 16], replicated, may hold values from -0.125 to 0.125
- state_rate: float32 [16], P('tp'), may hold values from 0 to 1, as said below
- state_jumps: float32 [32768, 16], P(('fs', 'sp'), 'tp'), parts along dimension 0, may hold values from -3 to 0
- state_gain: float32 [1024], P('tp'), may hold values from 0.1 to 1.9
- filter_value: bfloat16 [5, 1024], P(None, 'tp'), may hold values from -2.5 to 2.5
- filter_keys: bfloat16 [5, 1024], P(None, 'tp'), may hold values from -2.5 to 2.5
- filter_query: bfloat16 [5, 1024], P(None, 'tp'), may hold values from -2.5 to 2.5
- window_query: bfloat16 [2048, 2048], P('sp', 'tp'), may hold values from -64 to 64
- window_keys: bfloat16 [2048, 1024], P('sp', 'tp'), may hold values from -1 to 1
- window_values: bfloat16 [2048, 1024], P('sp', 'tp'), may hold values from -0.125 to 0.125
- window_sink: float32 [16], P('tp'), may hold values from 2.5 to 5.5
- state_output: bfloat16 [1024, 2048], P('tp', 'sp'), may hold values from -0.1875 to 0.1875
- window_output: bfloat16 [2048, 2048], P('tp', 'sp'), may hold values from -2 to 2
Outputs:
- mixed: bfloat16 [32768, 2048], P(('fs', 'sp', 'tp')), parts along dimension 0
The draws below stay inside these ranges and needn't reach their ends.
There are 4 independent parts, one for each index of `fs`. The reference program is written for one: setup_inputs(seed, part) draws one part's arguments, and reference() takes and returns one part's arrays. A program takes and returns all parts, laid end to end along the dimension named above; an argument that names none is the same for every part. Nothing has to cross between parts.
Inputs may be any that keep to these rules, and one draw needn't show every extreme that they name: `state_rate`: a positive rate for each head.
All inputs are finite; a program needn't handle non-finite values.
Results may differ from the reference program's by a relative error of at most 0.015.
The reference program's roundings to bfloat16 on the way count: a program that leaves them out, or rounds other values in their place, can miss the bound.
Values may be sent and summed in bfloat16 or wider, within the bound.
A program may use at most 64 MiB of HBM per device.

```python
import math
import jax
import jax.numpy as jnp
from jax import lax

D = 2048
MIXER_STATE_HEADS = 16
STATE_HEAD_DIM = 64
STATE_GROUPS = 8
STATE_SIZE = 128
WINDOW_HEADS = 16
WINDOW_KV_HEADS = 8
HEAD_DIM = 128
CONV_WIDTH = 5
WINDOW = 128
BLOCK = 128
GRID_WIDTH = 64
TOK_DEV = 512
SEQUENCE_LENGTH = 8192
STATE_INNER = 1024
GROUP_WIDTH = 1024
WINDOW_WIDTH = 2048
KV_WIDTH = 1024
N_TP = 8


def draw_state_rate(key, part):
    shuffled = jax.random.permutation(jax.random.fold_in(key, 101), MIXER_STATE_HEADS)
    quick_count = MIXER_STATE_HEADS // 2
    quick_heads = shuffled < quick_count
    quick_rate = jnp.exp(jax.random.uniform(jax.random.fold_in(key, 102), (MIXER_STATE_HEADS,), jnp.float32, math.log(1.0 / 60.0), math.log(1.0 / 20.0)))
    slow_rate = jax.random.uniform(jax.random.fold_in(key, 103), (MIXER_STATE_HEADS,), jnp.float32, 0.1, 0.4) / SEQUENCE_LENGTH
    return jnp.where(quick_heads, quick_rate, slow_rate).astype(jnp.float32)


def draw_state_jumps(key, part):
    block_count = SEQUENCE_LENGTH // TOK_DEV
    factors = jnp.exp(jax.random.uniform(jax.random.fold_in(key, 201), (block_count,), jnp.float32, math.log(0.5), math.log(2.5)))
    token_position = jnp.arange(SEQUENCE_LENGTH)
    baseline_level = -0.3 * jnp.take(factors, token_position // TOK_DEV) / SEQUENCE_LENGTH
    spike_positions = jax.random.randint(jax.random.fold_in(key, 202), (3,), 0, SEQUENCE_LENGTH)
    spike_count = (token_position[None, :] == spike_positions[:, None]).astype(jnp.float32)
    spike_depth = jnp.log(jax.random.uniform(jax.random.fold_in(key, 203), (3, MIXER_STATE_HEADS), jnp.float32, 0.5, 0.8))
    return (baseline_level[:, None] + jnp.dot(spike_count.T, spike_depth)).astype(jnp.float32)


def draw_tokens(key, part):
    rows = jnp.clip(jax.random.normal(jax.random.fold_in(key, 404), (SEQUENCE_LENGTH, D), jnp.float32), -6.0, 6.0)
    return rows.astype(jnp.bfloat16)


def window_pair(key):
    scale = 1.0 / math.sqrt(D)
    keys_all = jnp.clip(jax.random.normal(jax.random.fold_in(key, 306), (D, KV_WIDTH), jnp.float32), -6.0, 6.0) * scale
    query_all = jnp.clip(jax.random.normal(jax.random.fold_in(key, 307), (D, WINDOW_WIDTH), jnp.float32), -6.0, 6.0) * scale
    return (query_all.astype(jnp.float32), keys_all.astype(jnp.float32))


def draw_window_query(key, part):
    return window_pair(key)[0].astype(jnp.bfloat16)


def draw_window_keys(key, part):
    return window_pair(key)[1].astype(jnp.bfloat16)


def levels(rng, shape, split, smallest, top_value):
    def one(dim, parts):
        heights = jax.random.uniform(jax.random.fold_in(jax.random.fold_in(rng, 6), dim), (parts,), jnp.float32, smallest / len(split), top_value / len(split))
        return jnp.repeat(jnp.exp(heights), shape[dim] // parts).reshape((-1,) + (1,) * (len(shape) - dim - 1))

    factor_of = one(*split[0])
    for cut in split[1:]:
        factor_of = factor_of * one(*cut)
    return factor_of


def centred(rng, shape, scale, reach, cuts=(), kind=jnp.bfloat16):
    result = scale * jax.random.normal(rng, shape, jnp.float32)
    if cuts:
        result = result * levels(rng, shape, cuts, -0.22, 0.18)
    return jnp.clip(result, -reach, reach).astype(kind)


def setup_inputs(seed: int = 0, part: int = 0) -> dict:
    key_list = jax.random.split(jax.random.key(seed), 20)
    part_splits = jax.random.split(jax.random.fold_in(key_list[19], part), 20)
    return {
        "tokens": draw_tokens(jax.random.fold_in(jax.random.fold_in(key_list[19], part), 71), part),
        "norm_gain": jnp.clip(1.0 + 0.18 * jax.random.normal(key_list[1], (D,), jnp.float32), 0.1, 1.9),
        "state_gate": centred(key_list[2], (D, STATE_INNER), D ** -0.5, 0.125, ((0, 16), (1, 8))),
        "state_value": centred(key_list[3], (D, STATE_INNER), D ** -0.5, 0.125, ((0, 16), (1, 8))),
        "state_keys": centred(key_list[4], (D, GROUP_WIDTH), D ** -0.5, 0.125, ((0, 16), (1, 8))),
        "state_query": centred(key_list[5], (D, GROUP_WIDTH), D ** -0.5, 0.125, ((0, 16), (1, 8))),
        "state_step": centred(key_list[6], (D, MIXER_STATE_HEADS), D ** -0.5, 0.125),
        "state_rate": draw_state_rate(jax.random.fold_in(key_list[19], 71), part),
        "state_jumps": draw_state_jumps(jax.random.fold_in(jax.random.fold_in(key_list[19], part), 71), part),
        "state_gain": jnp.clip(1.0 + 0.18 * jax.random.normal(key_list[9], (STATE_INNER,), jnp.float32), 0.1, 1.9),
        "filter_value": centred(key_list[10], (CONV_WIDTH, STATE_INNER), CONV_WIDTH ** -0.5, 2.5, ((1, 8),)),
        "filter_keys": centred(key_list[11], (CONV_WIDTH, GROUP_WIDTH), CONV_WIDTH ** -0.5, 2.5, ((1, 8),)),
        "filter_query": centred(key_list[12], (CONV_WIDTH, GROUP_WIDTH), CONV_WIDTH ** -0.5, 2.5, ((1, 8),)),
        "window_query": draw_window_query(jax.random.fold_in(key_list[19], 71), part),
        "window_keys": draw_window_keys(jax.random.fold_in(key_list[19], 71), part),
        "window_values": centred(key_list[15], (D, KV_WIDTH), D ** -0.5, 0.125, ((0, 16), (1, 8))),
        "window_sink": jnp.clip(2.5 + 3.0 * jax.random.uniform(key_list[16], (WINDOW_HEADS,), jnp.float32) ** levels(key_list[16], (WINDOW_HEADS,), ((0, 8),), -0.2, 0.2), 2.5, 5.5),
        "state_output": centred(key_list[17], (STATE_INNER, D), STATE_INNER ** -0.5, 0.1875, ((0, 8), (1, 16))),
        "window_output": centred(key_list[18], (WINDOW_WIDTH, D), (WINDOW_WIDTH // (2 * WINDOW + 1)) ** -0.5, 2.0, ((0, 8), (1, 16))),
    }


def rotate_grid(vectors, positions, grid_width):
    head_dim = vectors.shape[-1]
    quarter = head_dim // 4
    half_dim = head_dim // 2
    inverse = 10000.0 ** (-jnp.arange(quarter, dtype=jnp.float32) / quarter)
    grid_row = (positions // grid_width).astype(jnp.float32)
    grid_col = (positions % grid_width).astype(jnp.float32)
    angle_row = grid_row[:, None] * inverse[None, :]
    angle_col = grid_col[:, None] * inverse[None, :]
    angles = jnp.concatenate([angle_row, angle_row, angle_col, angle_col], axis=-1)[:, None, :]
    first_half = vectors[..., :half_dim]
    second = vectors[..., half_dim:]
    turned = jnp.concatenate([-first_half[..., quarter:], first_half[..., :quarter], -second[..., quarter:], second[..., :quarter]], axis=-1)
    return (vectors.astype(jnp.float32) * jnp.cos(angles) + turned.astype(jnp.float32) * jnp.sin(angles)).astype(jnp.bfloat16)

def window_attend(query_rows, keys_pad, values_pad, sink_logits, key_start, total_len, window):
    row_count, query_heads, head_dim = query_rows.shape
    kv_heads = keys_pad.shape[1]
    group_size = query_heads // kv_heads
    block_count = row_count // window
    query_blocks = query_rows.reshape(block_count, window, kv_heads, group_size, head_dim)
    key_split = keys_pad.reshape(block_count + 2, window, kv_heads, head_dim)
    value_split = values_pad.reshape(block_count + 2, window, kv_heads, head_dim)
    key_band = jnp.concatenate([key_split[:-2], key_split[1:-1], key_split[2:]], axis=1)
    value_band = jnp.concatenate([value_split[:-2], value_split[1:-1], value_split[2:]], axis=1)
    scores = jnp.einsum('kihgd,kjhd->khgij', query_blocks.astype(jnp.float32), key_band.astype(jnp.float32)) * head_dim ** (-0.5)
    query_pos = jnp.arange(window)[:, None]
    band_pos = jnp.arange(3 * window)[None, :]
    within = jnp.abs(band_pos - window - query_pos) <= window
    key_pos = key_start + jnp.arange(block_count)[:, None] * window + jnp.arange(3 * window)[None, :]
    inside = (key_pos >= 0) & (key_pos < total_len)
    valid_pair = (within[None] & inside[:, None, :])[:, None, None]
    sink_logit = sink_logits.reshape(kv_heads, group_size)[None, :, :, None, None]
    masked = jnp.where(valid_pair, scores, -1e+30)
    ceiling = jnp.maximum(lax.optimization_barrier(jnp.max(masked, axis=-1, keepdims=True)), sink_logit)
    weights = jnp.where(valid_pair, jnp.exp(masked - ceiling), 0.0)
    denominator = jnp.exp(sink_logit - ceiling) + lax.optimization_barrier(jnp.sum(weights, axis=-1, keepdims=True))
    weights_bf = (weights / denominator).astype(jnp.bfloat16)
    mixed_rows = jnp.einsum('khgij,kjhd->kihgd', weights_bf.astype(jnp.float32), value_band.astype(jnp.float32))
    return mixed_rows.reshape(row_count, query_heads * head_dim).astype(jnp.bfloat16)

def block_terms(query_rows, key_rows, value_rows, log_rows, block_len):
    row_count, group_count, state_size = query_rows.shape
    head_ratio, head_dim = (value_rows.shape[2], value_rows.shape[3])
    block_count = row_count // block_len
    query_blocks = query_rows.reshape(block_count, block_len, group_count, state_size)
    key_blocks = key_rows.reshape(block_count, block_len, group_count, state_size)
    value_blocks = value_rows.reshape(block_count, block_len, group_count, head_ratio, head_dim)
    decay_cum = jnp.cumsum(log_rows.reshape(block_count, block_len, group_count, head_ratio), axis=1)
    decay_total = decay_cum[:, -1]
    gram_block = jnp.einsum('kign,kjgn->kgij', query_blocks.astype(jnp.float32), key_blocks.astype(jnp.float32))
    cum_heads = jnp.moveaxis(decay_cum, 1, 3)
    distance = jnp.abs(cum_heads[..., :, None] - cum_heads[..., None, :])
    pair_weight = (gram_block[:, :, None] * jnp.exp(-distance)).astype(jnp.bfloat16)
    near_terms = jnp.einsum('kgrij,kjgrp->kigrp', pair_weight.astype(jnp.float32), value_blocks.astype(jnp.float32))
    keys_after = (key_blocks[:, :, :, None, :] * jnp.exp(decay_total[:, None] - decay_cum)[..., None]).astype(jnp.bfloat16)
    keys_before = (key_blocks[:, :, :, None, :] * jnp.exp(decay_cum)[..., None]).astype(jnp.bfloat16)
    state_after = jnp.einsum('kjgrn,kjgrp->kgrnp', keys_after.astype(jnp.float32), value_blocks.astype(jnp.float32))
    state_before = jnp.einsum('kjgrn,kjgrp->kgrnp', keys_before.astype(jnp.float32), value_blocks.astype(jnp.float32))
    before = jnp.cumsum(decay_total, axis=0) - decay_total
    overall = lax.optimization_barrier(jnp.sum(decay_total, axis=0))
    after_sum = overall[None] - before - decay_total
    block_order = jnp.arange(block_count)
    earlier_mask = (block_order[None, :] < block_order[:, None])[:, :, None, None]
    later_mask = (block_order[None, :] > block_order[:, None])[:, :, None, None]
    gap_fwd = before[:, None] - before[None, :] - decay_total[None, :]
    gap_bwd = before[None, :] - before[:, None] - decay_total[:, None]
    weight_fwd = jnp.where(earlier_mask, jnp.exp(jnp.minimum(gap_fwd, 0.0)), 0.0)
    weight_bwd = jnp.where(later_mask, jnp.exp(jnp.minimum(gap_bwd, 0.0)), 0.0)
    carried_fwd = jnp.einsum('abgr,bgrnp->agrnp', weight_fwd, state_after, precision=lax.Precision.HIGHEST)
    carried_bwd = jnp.einsum('abgr,bgrnp->agrnp', weight_bwd, state_before, precision=lax.Precision.HIGHEST)
    summary_fwd = jnp.einsum('agr,agrnp->grnp', jnp.exp(after_sum), state_after, precision=lax.Precision.HIGHEST)
    summary_bwd = jnp.einsum('agr,agrnp->grnp', jnp.exp(before), state_before, precision=lax.Precision.HIGHEST)
    pieces = (near_terms, carried_fwd, carried_bwd, decay_cum, decay_total, before, after_sum, query_blocks)
    return (pieces, (summary_fwd, summary_bwd, overall))

def finish_terms(pieces, incoming_fwd, incoming_bwd):
    near_terms, carried_fwd, carried_bwd, decay_cum, decay_total, before, after_sum, query_blocks = pieces
    total_fwd = carried_fwd + jnp.exp(before)[..., None, None] * incoming_fwd[None]
    total_bwd = carried_bwd + jnp.exp(after_sum)[..., None, None] * incoming_bwd[None]
    query_wide = query_blocks.astype(jnp.float32)
    read_fwd = jnp.einsum('kign,kgrnp->kigrp', query_wide, total_fwd, precision=lax.Precision.HIGHEST)
    read_bwd = jnp.einsum('kign,kgrnp->kigrp', query_wide, total_bwd, precision=lax.Precision.HIGHEST)
    combined = near_terms + jnp.exp(decay_cum)[..., None] * read_fwd + jnp.exp(decay_total[:, None] - decay_cum)[..., None] * read_bwd
    block_count, block_len, group_count, head_ratio, head_dim = combined.shape
    return combined.reshape(block_count * block_len, group_count, head_ratio, head_dim)

def reference(tokens, norm_gain, state_gate, state_value, state_keys, state_query, state_step, state_rate, state_jumps, state_gain, filter_value, filter_keys, filter_query, window_query, window_keys, window_values, window_sink, state_output, window_output):
    length, feat_width = tokens.shape
    rows_wide = tokens.astype(jnp.float32)
    normed = (rows_wide * lax.rsqrt(lax.optimization_barrier(jnp.mean(rows_wide * rows_wide, axis=-1, keepdims=True)) + 1e-06) * norm_gain).astype(jnp.bfloat16)
    gate_rows = jnp.dot(normed, state_gate, preferred_element_type=jnp.float32).astype(jnp.bfloat16)
    value_pre = jnp.dot(normed, state_value, preferred_element_type=jnp.float32).astype(jnp.bfloat16)
    keys_pre = jnp.dot(normed, state_keys, preferred_element_type=jnp.float32).astype(jnp.bfloat16)
    query_pre = jnp.dot(normed, state_query, preferred_element_type=jnp.float32).astype(jnp.bfloat16)
    query_raw = jnp.dot(normed, window_query, preferred_element_type=jnp.float32).astype(jnp.bfloat16)
    keys_raw = jnp.dot(normed, window_keys, preferred_element_type=jnp.float32).astype(jnp.bfloat16)
    values_rows = jnp.dot(normed, window_values, preferred_element_type=jnp.float32).astype(jnp.bfloat16)
    step_rows = jax.nn.softplus(jnp.dot(normed, state_step, preferred_element_type=jnp.float32))
    log_decay = -state_rate[None, :] * step_rows + state_jumps
    half_width = filter_value.shape[0] // 2
    stacked = jnp.concatenate([value_pre, keys_pre, query_pre], axis=-1)
    padded = jnp.pad(stacked, ((half_width, half_width), (0, 0)))
    filters = jnp.concatenate([filter_value, filter_keys, filter_query], axis=-1).astype(jnp.float32)
    filtered = jnp.zeros(stacked.shape, jnp.float32)
    for offset in range(filters.shape[0]):
        filtered = filtered + padded[offset:offset + length].astype(jnp.float32) * filters[offset]
    value_cols = STATE_INNER
    key_cols = GROUP_WIDTH
    head_ratio = MIXER_STATE_HEADS // STATE_GROUPS
    inner_rows = jax.nn.silu(filtered[:, :value_cols]).reshape(length, MIXER_STATE_HEADS, STATE_HEAD_DIM) * step_rows[..., None]
    scan_values = inner_rows.astype(jnp.bfloat16).reshape(length, STATE_GROUPS, head_ratio, STATE_HEAD_DIM)
    scan_keys = filtered[:, value_cols:value_cols + key_cols].astype(jnp.bfloat16).reshape(length, STATE_GROUPS, STATE_SIZE)
    scan_query = filtered[:, value_cols + key_cols:].astype(jnp.bfloat16).reshape(length, STATE_GROUPS, STATE_SIZE)
    group_logs = log_decay.reshape(length, STATE_GROUPS, head_ratio)

    def one_group(group_args):
        group_query, group_keys, group_values, group_decay = group_args
        pieces, summaries = block_terms(group_query[:, None], group_keys[:, None], group_values[:, None], group_decay[:, None], BLOCK)
        zero_state = jnp.zeros((1, head_ratio, STATE_SIZE, STATE_HEAD_DIM), jnp.float32)
        return finish_terms(pieces, zero_state, zero_state)[:, 0]
    per_group = lax.map(one_group, (jnp.moveaxis(scan_query, 1, 0), jnp.moveaxis(scan_keys, 1, 0), jnp.moveaxis(scan_values, 1, 0), jnp.moveaxis(group_logs, 1, 0)))
    scan_out = jnp.moveaxis(per_group, 0, 1).reshape(length, STATE_INNER)
    gated_rows = scan_out * jax.nn.silu(gate_rows.astype(jnp.float32))
    per_head = gated_rows.reshape(length, MIXER_STATE_HEADS, STATE_HEAD_DIM)
    state_mix = (per_head * lax.rsqrt(lax.optimization_barrier(jnp.mean(per_head * per_head, axis=-1, keepdims=True)) + 1e-06) * state_gain.reshape(MIXER_STATE_HEADS, STATE_HEAD_DIM)).astype(jnp.bfloat16).reshape(length, STATE_INNER)
    positions = jnp.arange(length, dtype=jnp.int32)
    query_rot = rotate_grid(query_raw.reshape(length, WINDOW_HEADS, HEAD_DIM), positions, GRID_WIDTH)
    keys_rot = rotate_grid(keys_raw.reshape(length, WINDOW_KV_HEADS, HEAD_DIM), positions, GRID_WIDTH)
    keys_pad = jnp.pad(keys_rot, ((WINDOW, WINDOW), (0, 0), (0, 0)))
    values_pad = jnp.pad(values_rows.reshape(length, WINDOW_KV_HEADS, HEAD_DIM), ((WINDOW, WINDOW), (0, 0), (0, 0)))
    group_size = WINDOW_HEADS // WINDOW_KV_HEADS

    def one_head(head_args):
        head_query, head_keys, head_values, head_sink = head_args
        return window_attend(head_query, head_keys[:, None], head_values[:, None], head_sink, -WINDOW, length, WINDOW)
    per_kv = lax.map(one_head, (jnp.moveaxis(query_rot.reshape(length, WINDOW_KV_HEADS, group_size, HEAD_DIM), 1, 0), jnp.moveaxis(keys_pad, 1, 0), jnp.moveaxis(values_pad, 1, 0), window_sink.reshape(WINDOW_KV_HEADS, group_size)))
    window_mix = jnp.moveaxis(per_kv, 0, 1).reshape(length, WINDOW_WIDTH)
    state_cols = STATE_INNER // N_TP
    window_cols = WINDOW_WIDTH // N_TP

    def add_group(group_index, running):
        state_start = (group_index * state_cols).astype(jnp.int32)
        window_start = (group_index * window_cols).astype(jnp.int32)
        state_part = lax.dynamic_slice_in_dim(state_mix, state_start, state_cols, 1)
        state_weight = lax.dynamic_slice_in_dim(state_output, state_start, state_cols, 0)
        window_part = lax.dynamic_slice_in_dim(window_mix, window_start, window_cols, 1)
        window_weight = lax.dynamic_slice_in_dim(window_output, window_start, window_cols, 0)
        term_rows = jnp.dot(state_part, state_weight, preferred_element_type=jnp.float32) + jnp.dot(window_part, window_weight, preferred_element_type=jnp.float32)
        rounded = lax.optimization_barrier(term_rows.astype(jnp.bfloat16))
        return running + rounded.astype(jnp.float32)
    summed = lax.fori_loop(0, N_TP, add_group, jnp.zeros((length, feat_width), jnp.float32))
    return summed.astype(jnp.bfloat16)
```

```python
import functools

import jax
import jax.numpy as jnp
from jax import lax
from jax.experimental import pallas as pl
from jax.experimental.pallas import tpu as pltpu
from jax.sharding import PartitionSpec as P

BLOCK = 128
LANES = 128
HALO = 16
GRID_WIDTH = 64
QUARTER = 32
WIN_COLS = 1024
F32 = jnp.float32
BF16 = jnp.bfloat16
HIGHEST = lax.Precision.HIGHEST


def modulo(value, count):
    return lax.rem(value + 2 * count, count)


def half_lanes(shape):
    return lax.broadcasted_iota(jnp.int32, shape, 1) < LANES // 2


def dot(a, b, precision=None):
    return jnp.dot(a, b, preferred_element_type=F32, precision=precision)


def kernel(
    n,
    ny,
    nx,
    tokens,
    norm_gain,
    gate_w,
    value_w,
    keys_w,
    query_w,
    step_w,
    rate,
    jumps,
    gain,
    filter_value,
    filter_keys,
    filter_query,
    wq_w,
    wk_w,
    wv_w,
    sink,
    out_state_w,
    out_window_w,
    result,
    win,
    wout,
    normed,
    acc,
    halo_in,
    pre,
    cos_t,
    sin_t,
    step_b,
    cum_b,
    step_cols,
    scan_v,
    scan_k,
    scan_q,
    query_rot,
    kv_ext,
    state_a,
    state_c,
    carry_f,
    carry_b,
    scan_loc,
    message,
    arrived,
    totals_out,
    totals,
    incoming,
    income_out,
    mix,
    pair_out,
    pair_in,
    own_part,
    group_out,
    group_in,
    load_sem,
    zs,
    zr,
    ys,
    yr,
    hs,
    hr,
    ks,
    kr,
    a1s,
    a1r,
    a2s,
    a2r,
    ts,
    tr,
    ps,
    pr,
    gs,
    gr,
):
    rows = tokens.shape[0]
    blocks = rows // BLOCK
    depth = tokens.shape[1]
    shard = depth // n
    me = lax.axis_index("sp")
    my_y = lax.axis_index("fs")
    my_tp = lax.axis_index("tp")
    core = lax.rem(my_tp, 2)
    my_x = my_tp // 2
    right, left = modulo(me + 1, n), modulo(me - 1, n)
    up, down = modulo(my_y + 1, ny), modulo(my_y - 1, ny)
    partner = my_tp + 1 - 2 * core
    own_half = lax.rem(my_y, 2)
    half = n // 2

    loads = []
    column = 0
    for k, ref in enumerate((value_w, keys_w, query_w, gate_w, wq_w, wk_w, wv_w)):
        width = ref.shape[1]
        loads.append(
            pltpu.make_async_copy(
                ref, win.at[me, :, pl.ds(column, width)], load_sem.at[k]
            )
        )
        column += width
    loads.append(
        pltpu.make_async_copy(out_state_w, wout.at[me, pl.ds(0, LANES), :], load_sem.at[7])
    )
    loads.append(
        pltpu.make_async_copy(
            out_window_w, wout.at[me, pl.ds(LANES, 2 * LANES), :], load_sem.at[8]
        )
    )
    for load in loads:
        load.start()

    barrier = pltpu.get_barrier_semaphore()
    peers = [{"sp": modulo(me + o, n)} for o in range(1, n)]
    peers += [{"fs": modulo(my_y + o, ny)} for o in sorted({1, ny - 1})]
    peers += [{"tp": partner}]
    peers += [{"tp": 2 * modulo(my_x + o, nx) + core} for o in range(1, nx)]
    for peer in peers:
        pl.semaphore_signal(barrier, inc=1, device_id=peer)
    for load in loads:
        load.wait()
    pl.semaphore_wait(barrier, len(peers))

    def halo_copy(d):
        source = tokens.at[pl.ds(rows - HALO, HALO)] if d == 0 else tokens.at[pl.ds(0, HALO)]
        return pltpu.make_async_remote_copy(
            source,
            halo_in.at[d],
            hs.at[d],
            hr.at[d],
            device_id={"sp": right if d == 0 else left},
        )

    buffers = (win, wout)

    def part(k, source, which, q):
        size = buffers[k].shape[1] // 4
        start = pl.multiple_of((2 * which + q) * size, size)
        return buffers[k].at[source, pl.ds(start, size)]

    def origin(d, s):
        return modulo(me - s, n) if d == 0 else modulo(me + s, n)

    def z_copy(d, s, k, q):
        ref = part(k, origin(d, s - 1), own_half, q)
        return pltpu.make_async_remote_copy(
            ref,
            ref,
            zs.at[d, s - 1, 2 * k + q],
            zr.at[d, s - 1, 2 * k + q],
            device_id={"sp": right if d == 0 else left},
        )

    def z_arrival(d, s, k, q):
        ref = part(k, origin(d, s), own_half, q)
        return pltpu.make_async_remote_copy(
            ref,
            ref,
            zs.at[d, s - 1, 2 * k + q],
            zr.at[d, s - 1, 2 * k + q],
            device_id={"sp": right if d == 0 else left},
        )

    def y_copy(d, s, k, q, which):
        ref = part(k, origin(d, s), which, q)
        return pltpu.make_async_remote_copy(
            ref,
            ref,
            ys.at[d, s - 1, 2 * k + q],
            yr.at[d, s - 1, 2 * k + q],
            device_id={"fs": up if q == 0 else down},
        )

    for d in range(2):
        halo_copy(d).start()
    for k in range(2):
        for q in range(2):
            for d in range(2):
                if half > 1 or q == d:
                    z_copy(d, 1, k, q).start()

    def normalise(x):
        wide = x.astype(F32)
        scale = lax.rsqrt(jnp.mean(wide * wide, axis=-1, keepdims=True) + 1e-06)
        return (wide * scale * norm_gain[...]).astype(BF16)

    def normalise_chunk(i, carry):
        start = pl.multiple_of(i * 32, 32)
        normed[pl.ds(HALO + start, 32), :] = normalise(tokens[pl.ds(start, 32), :])
        return carry

    lax.fori_loop(0, rows // 32, normalise_chunk, 0)
    for d in range(2):
        halo_copy(d).wait_recv()
        normed[(0 if d == 0 else HALO + rows) : (HALO if d == 0 else 2 * HALO + rows), :] = (
            normalise(halo_in[d])
        )

    def project(source, first):
        x = normed[:, pl.ds(pl.multiple_of(source * shard, shard), shard)]
        for c in range(0, WIN_COLS, 256):
            term = dot(x, win[source, :, c : c + 256])
            if first:
                acc[:, c : c + 256] = term
            else:
                acc[:, c : c + 256] += term

    project(me, True)

    heads = lax.broadcasted_iota(jnp.int32, (step_w.shape[1], LANES), 0)
    lanes_of = lax.broadcasted_iota(jnp.int32, (step_w.shape[1], LANES), 1)
    spread = (heads == 2 * my_tp + lanes_of // (LANES // 2)).astype(BF16)
    step_cols[...] = dot(step_w[...], spread).astype(BF16)
    tri = (
        lax.broadcasted_iota(jnp.int32, (BLOCK, BLOCK), 0)
        >= lax.broadcasted_iota(jnp.int32, (BLOCK, BLOCK), 1)
    ).astype(F32)
    first_head = half_lanes((1, LANES))

    def decay_block(b):
        start = pl.multiple_of(b * BLOCK, BLOCK)
        raw = dot(normed[pl.ds(HALO + start, BLOCK), :], step_cols[...])
        step = jnp.maximum(raw, 0.0) + jnp.log1p(jnp.exp(-jnp.abs(raw)))
        rate_row = jnp.where(first_head, rate[0], rate[1])
        jump = jumps[pl.ds(start, BLOCK), :]
        logs = -rate_row * step + jnp.where(first_head, jump[:, 0:1], jump[:, 1:2])
        step_b[pl.ds(start, BLOCK), :] = step
        cum_b[pl.ds(start, BLOCK), :] = dot(tri, logs, HIGHEST)

    angle_rows = rows // half

    def angle_block(i):
        start = pl.multiple_of(i * angle_rows, angle_rows)
        lane = lax.broadcasted_iota(jnp.int32, (angle_rows, LANES), 1)
        position = (
            lax.broadcasted_iota(jnp.int32, (angle_rows, LANES), 0) + me * rows + start
        )
        row_at = (position // GRID_WIDTH).astype(F32)
        col_at = lax.rem(position, GRID_WIDTH).astype(F32)
        exponent = lax.rem(lane, QUARTER).astype(F32) / -QUARTER
        inverse = jnp.exp(exponent[0:8] * 9.210340371976184)[0:1]
        angle = jnp.where(lane < LANES // 2, row_at, col_at) * inverse
        sine = jnp.sin(angle)
        cos_t[pl.ds(start, angle_rows), :] = jnp.cos(angle)
        sin_t[pl.ds(start, angle_rows), :] = jnp.where(
            lax.rem(lane, 2 * QUARTER) < QUARTER, -sine, sine
        )

    other_half = 1 - own_half

    def gather_step(s, carry):
        @pl.when(s < half)
        def _():
            for k in range(2):
                for q in range(2):
                    for d in range(2):
                        z_arrival(d, s, k, q).wait_recv()
                        if q == d:
                            z_copy(d, s + 1, k, q).start()
                        else:

                            @pl.when(s + 1 < half)
                            def _():
                                z_copy(d, s + 1, k, q).start()

                        y_copy(d, s, k, q, own_half).start()

        @pl.when(s == half)
        def _():
            for k in range(2):
                for d in range(2):
                    z_arrival(d, s, k, d).wait_recv()
                    y_copy(d, s, k, d, own_half).start()

        @pl.when(s <= half)
        def _():
            angle_block(s - 1)

        @pl.when(s <= blocks)
        def _():
            decay_block(s - 1)

        before = s - 1

        @pl.when((before >= 1) & (before < half))
        def _():
            for d in range(2):
                for q in range(2):
                    y_copy(d, before, 0, q, other_half).wait_recv()
            for d in range(2):
                project(origin(d, before), False)

        @pl.when(before == half)
        def _():
            for d in range(2):
                y_copy(d, before, 0, d, other_half).wait_recv()
            project(origin(0, before), False)

        return carry

    lax.fori_loop(1, half + 2, gather_step, 0)
    for b in range(half, blocks):
        if b > half:
            decay_block(b)

    def rotate(x, b):
        start = pl.multiple_of(b * BLOCK, BLOCK)
        wide = x.astype(BF16).astype(F32)
        lane = lax.broadcasted_iota(jnp.int32, (BLOCK, LANES), 1)
        turned = jnp.where(
            lax.rem(lane, 2 * QUARTER) < QUARTER,
            pltpu.roll(wide, LANES - QUARTER, 1),
            pltpu.roll(wide, QUARTER, 1),
        )
        return (
            wide * cos_t[pl.ds(start, BLOCK), :] + turned * sin_t[pl.ds(start, BLOCK), :]
        ).astype(BF16)

    def key_block(b, carry):
        start = pl.multiple_of(b * BLOCK, BLOCK)
        own = pl.ds(HALO + start, BLOCK)
        target = pl.ds(BLOCK + start, BLOCK)
        kv_ext[target, 0:LANES] = rotate(acc[own, 768:896], b)
        kv_ext[target, LANES : 2 * LANES] = acc[own, 896:1024].astype(BF16)
        return carry

    def query_block(b, carry):
        start = pl.multiple_of(b * BLOCK, BLOCK)
        own = pl.ds(HALO + start, BLOCK)
        for h in range(2):
            query_rot[pl.ds(start, BLOCK), h * LANES : (h + 1) * LANES] = rotate(
                acc[own, 512 + h * LANES : 512 + (h + 1) * LANES], b
            )
        return carry

    lax.fori_loop(0, blocks, key_block, 0)

    def kv_copy(d):
        source = kv_ext.at[pl.ds(rows if d == 0 else BLOCK, BLOCK)]
        return pltpu.make_async_remote_copy(
            source,
            kv_ext.at[pl.ds(0 if d == 0 else rows + BLOCK, BLOCK)],
            ks.at[d],
            kr.at[d],
            device_id={"sp": right if d == 0 else left},
        )

    pre[...] = acc[:, 0:384].astype(BF16).astype(F32)

    @pl.when(me == 0)
    def _():
        pre[0:HALO, :] = jnp.zeros((HALO, 384), F32)

    @pl.when(me == n - 1)
    def _():
        pre[HALO + rows : 2 * HALO + rows, :] = jnp.zeros((HALO, 384), F32)

    for d in range(2):
        kv_copy(d).start()

    taps = [f[...].astype(F32) for f in (filter_value, filter_keys, filter_query)]
    for b in range(blocks):
        for c in range(3):
            total = jnp.zeros((BLOCK, LANES), F32)
            for j in range(5):
                at = HALO + b * BLOCK + j - 2
                total = total + (
                    pre[at : at + BLOCK, c * LANES : (c + 1) * LANES] * taps[c][j : j + 1, :]
                )
            here = slice(b * BLOCK, (b + 1) * BLOCK)
            if c == 0:
                scan_v[here, :] = total * jax.nn.sigmoid(total) * step_b[here, :]
            elif c == 1:
                scan_k[here, :] = total.astype(BF16)
            else:
                scan_q[here, :] = total.astype(BF16)

    def block_states(b, carry):
        start = pl.multiple_of(b * BLOCK, BLOCK)
        here = pl.ds(start, BLOCK)
        cum = cum_b[here, :]
        total = cum[BLOCK - 1 : BLOCK, :]
        values = scan_v[here, :].astype(BF16).astype(F32)
        keys_t = scan_k[here, :].astype(F32).T.astype(BF16)
        state_a[b] = dot(keys_t, (values * jnp.exp(total - cum)).astype(BF16))
        state_c[b] = dot(keys_t, (values * jnp.exp(cum)).astype(BF16))
        return carry

    lax.fori_loop(0, blocks, block_states, 0)
    ends = [cum_b[(b + 1) * BLOCK - 1 : (b + 1) * BLOCK, :] for b in range(blocks)]
    forward = jnp.zeros((BLOCK, LANES), F32)
    for b in range(blocks):
        carry_f[b] = forward.astype(BF16)
        forward = forward * jnp.exp(ends[b]) + state_a[b]
    backward = jnp.zeros((BLOCK, LANES), F32)
    for b in reversed(range(blocks)):
        carry_b[b] = backward.astype(BF16)
        backward = backward * jnp.exp(ends[b]) + state_c[b]
    overall = functools.reduce(jnp.add, ends)

    piece = BLOCK // n
    message[...] = jnp.concatenate(
        [forward.reshape(n, piece, LANES), backward.reshape(n, piece, LANES)], axis=1
    ).astype(BF16)
    totals_out[...] = overall
    totals[me] = overall
    arrived[me] = message[me]

    def first_exchange(o):
        to = modulo(me + o, n)
        return (
            pltpu.make_async_remote_copy(
                message.at[to], arrived.at[me], a1s.at[o], a1r.at[o], device_id={"sp": to}
            ),
            pltpu.make_async_remote_copy(
                totals_out, totals.at[me], ts.at[o], tr.at[o], device_id={"sp": to}
            ),
        )

    def first_arrival(o):
        source = modulo(me - o, n)
        return (
            pltpu.make_async_remote_copy(
                arrived.at[source], arrived.at[source], a1s.at[o], a1r.at[o], device_id={"sp": source}
            ),
            pltpu.make_async_remote_copy(
                totals.at[source], totals.at[source], ts.at[o], tr.at[o], device_id={"sp": source}
            ),
        )

    order = sorted(range(1, n), key=lambda o: -min(o, n - o))
    for o in order:
        for copy in first_exchange(o):
            copy.start()

    near_mask = half_lanes((BLOCK, LANES))

    def local_scan(b, carry):
        start = pl.multiple_of(b * BLOCK, BLOCK)
        here = pl.ds(start, BLOCK)
        cum = cum_b[here, :]
        cum_t = cum.T
        total = cum[BLOCK - 1 : BLOCK, :]
        values = scan_v[here, :].astype(BF16)
        query = scan_q[here, :]
        gram = lax.dot_general(
            query, scan_k[here, :], (((1,), (1,)), ((), ())), preferred_element_type=F32
        )
        near = []
        for h in range(2):
            lane = h * (LANES // 2)
            gap = jnp.abs(cum[:, lane : lane + 1] - cum_t[lane : lane + 1, :])
            near.append(dot((gram * jnp.exp(-gap)).astype(BF16), values))
        out = jnp.where(near_mask, near[0], near[1])
        out += jnp.exp(cum) * dot(query, carry_f[b])
        out += jnp.exp(total - cum) * dot(query, carry_b[b])
        scan_loc[here, :] = out
        return carry

    lax.fori_loop(0, blocks, local_scan, 0)

    for o in order:
        for copy in first_arrival(o):
            copy.wait_recv()

    running = jnp.zeros((piece, LANES), F32)
    ahead = []
    for d in range(n):
        ahead.append(running)
        running = running * jnp.exp(totals[d]) + arrived[d].astype(F32)[0:piece]
    running = jnp.zeros((piece, LANES), F32)
    behind = [None] * n
    for d in reversed(range(n)):
        behind[d] = running
        running = running * jnp.exp(totals[d]) + arrived[d].astype(F32)[piece : 2 * piece]
    for d in range(n):
        income_out[d] = jnp.concatenate([ahead[d], behind[d]], axis=0).astype(BF16)
    incoming[me] = income_out[me]

    def second_exchange(o):
        to = modulo(me + o, n)
        return pltpu.make_async_remote_copy(
            income_out.at[to], incoming.at[me], a2s.at[o], a2r.at[o], device_id={"sp": to}
        )

    def second_arrival(o):
        source = modulo(me - o, n)
        return pltpu.make_async_remote_copy(
            incoming.at[source], incoming.at[source], a2s.at[o], a2r.at[o], device_id={"sp": source}
        )

    for o in order:
        second_exchange(o).start()

    lax.fori_loop(0, blocks, query_block, 0)
    for d in range(2):
        kv_copy(d).wait_recv()

    def attend(b, carry):
        start = pl.multiple_of(b * BLOCK, BLOCK)
        band = kv_ext[pl.ds(start, 3 * BLOCK), :]
        row = lax.broadcasted_iota(jnp.int32, (BLOCK, 3 * BLOCK), 0)
        col = lax.broadcasted_iota(jnp.int32, (BLOCK, 3 * BLOCK), 1)
        where_key = me * rows - BLOCK + start + col
        valid = (
            (jnp.abs(col - BLOCK - row) <= BLOCK) & (where_key >= 0) & (where_key < n * rows)
        )
        for h in range(2):
            query = query_rot[pl.ds(start, BLOCK), h * LANES : (h + 1) * LANES]
            scores = lax.dot_general(
                query, band[:, 0:LANES], (((1,), (1,)), ((), ())), preferred_element_type=F32
            ) * LANES ** (-0.5)
            masked = jnp.where(valid, scores, -1e30)
            ceiling = jnp.maximum(jnp.max(masked, axis=-1, keepdims=True), sink[h])
            weights = jnp.where(valid, jnp.exp(masked - ceiling), 0.0)
            bottom = jnp.exp(sink[h] - ceiling) + jnp.sum(weights, axis=-1, keepdims=True)
            probs = (weights / bottom).astype(BF16)
            mix[pl.ds(start, BLOCK), (1 + h) * LANES : (2 + h) * LANES] = dot(
                probs, band[:, LANES : 2 * LANES]
            ).astype(BF16)
        return carry

    lax.fori_loop(0, blocks, attend, 0)

    for o in order:
        second_arrival(o).wait_recv()
    incomes = incoming[...].astype(F32)
    income_f = incomes[:, 0:piece].reshape(BLOCK, LANES).astype(BF16)
    income_b = incomes[:, piece : 2 * piece].reshape(BLOCK, LANES).astype(BF16)
    befores = [jnp.zeros((1, LANES), F32)]
    for b in range(blocks):
        befores.append(befores[-1] + ends[b])
    for b in range(blocks):
        here = slice(b * BLOCK, (b + 1) * BLOCK)
        cum = cum_b[here, :]
        query = scan_q[here, :]
        after = overall - befores[b + 1]
        out = scan_loc[here, :]
        out += jnp.exp(cum + befores[b]) * dot(query, income_f)
        out += jnp.exp(ends[b] - cum + after) * dot(query, income_b)
        gate = acc[HALO + b * BLOCK : HALO + (b + 1) * BLOCK, 384:512].astype(BF16).astype(F32)
        gated = out * (gate * jax.nn.sigmoid(gate))
        square = gated * gated
        low = jnp.sum(jnp.where(near_mask, square, 0.0), axis=-1, keepdims=True)
        high = jnp.sum(jnp.where(near_mask, 0.0, square), axis=-1, keepdims=True)
        mean = jnp.where(near_mask, low, high) * (2.0 / LANES)
        mix[here, 0:LANES] = (gated * lax.rsqrt(mean + 1e-06) * gain[...]).astype(BF16)

    def wait_out(s, carry):
        @pl.when(s < half)
        def _():
            for d in range(2):
                for q in range(2):
                    y_copy(d, s, 1, q, other_half).wait_recv()

        @pl.when(s == half)
        def _():
            for d in range(2):
                y_copy(d, s, 1, d, other_half).wait_recv()

        return carry

    lax.fori_loop(1, half + 1, wait_out, 0)
    unit = rows // (2 * nx)

    def rows_for(c):
        return jnp.concatenate(
            [
                mix[pl.ds(pl.multiple_of((2 * x + c) * unit, unit), unit), :]
                for x in range(nx)
            ],
            axis=0,
        )

    def product(lhs, i):
        weights = jnp.concatenate([wout[2 * i], wout[2 * i + 1]], axis=1)
        return dot(lhs, weights).reshape(nx, unit, 2 * LANES)

    def other_product(i, carry):
        columns = pl.ds(pl.multiple_of(i * 2 * LANES, 2 * LANES), 2 * LANES)
        pair_out[:, :, columns] = product(rows_for(1 - core), i).astype(BF16)
        return carry

    def own_product(i, carry):
        columns = pl.ds(pl.multiple_of(i * 2 * LANES, 2 * LANES), 2 * LANES)
        own_part[:, :, columns] = product(rows_for(core), i)
        return carry

    def pair_copy(x):
        return pltpu.make_async_remote_copy(
            pair_out.at[x], pair_in.at[x], ps.at[x], pr.at[x], device_id={"tp": partner}
        )

    lax.fori_loop(0, n // 2, other_product, 0)
    for x in range(nx):
        pair_copy(x).start()
    lax.fori_loop(0, n // 2, own_product, 0)
    for x in range(nx):
        pair_copy(x).wait_recv()

    def group_copy(o):
        to = modulo(my_x + o, nx)
        return pltpu.make_async_remote_copy(
            group_out.at[o - 1],
            group_in.at[o - 1],
            gs.at[o - 1],
            gr.at[o - 1],
            device_id={"tp": 2 * to + core},
        )

    def group_sum(o):
        to = modulo(my_x + o, nx)
        return own_part[to] + pair_in[to].astype(F32)

    x_order = sorted(range(1, nx), key=lambda o: -min(o, nx - o))
    for o in x_order:
        group_out[o - 1] = group_sum(o).astype(BF16)
        group_copy(o).start()
    mine = group_sum(0)
    for o in x_order:
        group_copy(o).wait_recv()
        mine = mine + group_in[o - 1].astype(F32)
    result[...] = mine.astype(BF16)

    for d in range(2):
        halo_copy(d).wait_send()
        kv_copy(d).wait_send()
    for o in order:
        for copy in first_exchange(o):
            copy.wait_send()
        second_exchange(o).wait_send()
    for x in range(nx):
        pair_copy(x).wait_send()
    for o in x_order:
        group_copy(o).wait_send()

    def drain(s, carry):
        for k in range(2):
            for q in range(2):
                for d in range(2):
                    if q == d:
                        z_copy(d, s, k, q).wait_send()
                        y_copy(d, s, k, q, own_half).wait_send()
                    else:

                        @pl.when(s < half)
                        def _():
                            z_copy(d, s, k, q).wait_send()
                            y_copy(d, s, k, q, own_half).wait_send()

        return carry

    lax.fori_loop(1, half + 1, drain, 0)


def solution(mesh):
    n, ny, nt = (mesh.shape[a] for a in ("sp", "fs", "tp"))
    nx = nt // 2

    def shards(*args):
        args = list(args)
        rows, depth = args[0].shape
        args[1] = args[1].reshape(1, -1)
        args[9] = args[9].reshape(1, -1)
        shard = depth // n
        half = n // 2
        blocks = rows // BLOCK
        piece = BLOCK // n
        unit = rows // (2 * nx)
        vmem = pl.BlockSpec(memory_space=pltpu.VMEM)
        smem = pl.BlockSpec(memory_space=pltpu.SMEM)
        anywhere = pl.BlockSpec(memory_space=pl.ANY)
        specs = [vmem] * 19
        specs[7] = specs[16] = smem
        for i in (2, 3, 4, 5, 13, 14, 15, 17, 18):
            specs[i] = anywhere
        dma = pltpu.SemaphoreType.DMA
        V = pltpu.VMEM
        scratch = [
            V((n, shard, WIN_COLS), BF16),
            V((n, 3 * LANES, LANES), BF16),
            V((rows + 2 * HALO, depth), BF16),
            V((rows + 2 * HALO, WIN_COLS), F32),
            V((2, HALO, depth), BF16),
            V((rows + 2 * HALO, 3 * LANES), F32),
            V((rows, LANES), F32),
            V((rows, LANES), F32),
            V((rows, LANES), F32),
            V((rows, LANES), F32),
            V((depth, LANES), BF16),
            V((rows, LANES), F32),
            V((rows, LANES), BF16),
            V((rows, LANES), BF16),
            V((rows, 2 * LANES), BF16),
            V((rows + 2 * BLOCK, 2 * LANES), BF16),
            V((blocks, BLOCK, LANES), F32),
            V((blocks, BLOCK, LANES), F32),
            V((blocks, BLOCK, LANES), BF16),
            V((blocks, BLOCK, LANES), BF16),
            V((rows, LANES), F32),
            V((n, 2 * piece, LANES), BF16),
            V((n, 2 * piece, LANES), BF16),
            V((1, LANES), F32),
            V((n, 1, LANES), F32),
            V((n, 2 * piece, LANES), BF16),
            V((n, 2 * piece, LANES), BF16),
            V((rows, 3 * LANES), BF16),
            V((nx, unit, depth), BF16),
            V((nx, unit, depth), BF16),
            V((nx, unit, depth), F32),
            V((max(nx - 1, 1), unit, depth), BF16),
            V((max(nx - 1, 1), unit, depth), BF16),
            dma((9,)),
            dma((2, half, 4)),
            dma((2, half, 4)),
            dma((2, half, 4)),
            dma((2, half, 4)),
            dma((2,)),
            dma((2,)),
            dma((2,)),
            dma((2,)),
            dma((n,)),
            dma((n,)),
            dma((n,)),
            dma((n,)),
            dma((n,)),
            dma((n,)),
            dma((nx,)),
            dma((nx,)),
            dma((max(nx - 1, 1),)),
            dma((max(nx - 1, 1),)),
        ]
        return pl.pallas_call(
            functools.partial(kernel, n, ny, nx),
            out_shape=jax.ShapeDtypeStruct((rows // nt, depth), BF16),
            in_specs=specs,
            out_specs=vmem,
            scratch_shapes=scratch,
            compiler_params=pltpu.CompilerParams(
                collective_id=0, has_side_effects=True, vmem_limit_bytes=60 * 1024 * 1024
            ),
        )(*args)

    placed = (
        P(("fs", "sp"), None),
        P(),
        P("sp", "tp"),
        P("sp", "tp"),
        P("sp", "tp"),
        P("sp", "tp"),
        P(),
        P("tp"),
        P(("fs", "sp"), "tp"),
        P("tp"),
        P(None, "tp"),
        P(None, "tp"),
        P(None, "tp"),
        P("sp", "tp"),
        P("sp", "tp"),
        P("sp", "tp"),
        P("tp"),
        P("tp", "sp"),
        P("tp", "sp"),
    )
    return jax.shard_map(
        shards, mesh=mesh, in_specs=placed, out_specs=P(("fs", "sp", "tp"), None), check_vma=False
    )
```

```python
import functools

import jax
import jax.numpy as jnp
from jax import lax
from jax.experimental import pallas as pl
from jax.experimental.pallas import tpu as pltpu
from jax.sharding import PartitionSpec as P

BLOCK = 128
LANES = 128
HALO = 16
GRID_WIDTH = 64
QUARTER = 32
WIN_COLS = 1024
PIECES = 4
OUT_EARLY = 3
F32 = jnp.float32
BF16 = jnp.bfloat16
HIGHEST = lax.Precision.HIGHEST


def modulo(value, count):
    return lax.rem(value + 2 * count, count)


def half_lanes(shape):
    return lax.broadcasted_iota(jnp.int32, shape, 1) < LANES // 2


def dot(a, b, precision=None):
    return jnp.dot(a, b, preferred_element_type=F32, precision=precision)


def kernel(
    n,
    ny,
    nx,
    tokens_h,
    norm_gain_h,
    gate_w,
    value_w,
    keys_w,
    query_w,
    step_h,
    rate_h,
    jumps_h,
    gain_h,
    filter_value_h,
    filter_keys_h,
    filter_query_h,
    wq_w,
    wk_w,
    wv_w,
    sink_h,
    out_state_w,
    out_window_w,
    result,
    tokens,
    norm_gain,
    step_w,
    rate,
    jumps,
    gain,
    filter_value,
    filter_keys,
    filter_query,
    sink,
    win,
    wout,
    normed,
    acc,
    halo_in,
    pre,
    cos_t,
    sin_t,
    step_b,
    cum_b,
    step_cols,
    scan_v,
    scan_k,
    scan_q,
    query_rot,
    kv_ext,
    state_a,
    state_c,
    carry_f,
    carry_b,
    scan_loc,
    message,
    arrived,
    totals_out,
    totals,
    incoming,
    income_out,
    mix,
    part_sum,
    pair_out,
    pair_in,
    via_out,
    via_in,
    direct_out,
    direct_in,
    merged_out,
    merged_in,
    load_sem,
    zs,
    zr,
    ys,
    yr,
    czs,
    czr,
    cys,
    cyr,
    hs,
    hr,
    ks,
    kr,
    a1s,
    a1r,
    a2s,
    a2r,
    ts,
    tr,
    ps,
    pr,
    gs,
    gr,
):
    rows = tokens.shape[0]
    blocks = rows // BLOCK
    depth = tokens.shape[1]
    shard = depth // n
    me = lax.axis_index("sp")
    my_y = lax.axis_index("fs")
    my_tp = lax.axis_index("tp")
    core = lax.rem(my_tp, 2)
    my_x = my_tp // 2
    right, left = modulo(me + 1, n), modulo(me - 1, n)
    up, down = modulo(my_y + 1, ny), modulo(my_y - 1, ny)
    partner = my_tp + 1 - 2 * core
    own_half = lax.rem(my_y, 2)
    half = n // 2

    loads = []
    column = 0
    for k, ref in enumerate((value_w, keys_w, query_w, gate_w, wq_w, wk_w, wv_w)):
        width = ref.shape[1]
        loads.append(
            pltpu.make_async_copy(ref, win.at[me, :, pl.ds(column, width)], load_sem.at[k])
        )
        column += width
    late_loads = [
        pltpu.make_async_copy(tokens_h, tokens, load_sem.at[9]),
        pltpu.make_async_copy(norm_gain_h, norm_gain, load_sem.at[10]),
        pltpu.make_async_copy(step_h, step_w, load_sem.at[11]),
        pltpu.make_async_copy(rate_h, rate, load_sem.at[12]),
        pltpu.make_async_copy(jumps_h, jumps, load_sem.at[13]),
        pltpu.make_async_copy(gain_h, gain, load_sem.at[14]),
        pltpu.make_async_copy(filter_value_h, filter_value, load_sem.at[15]),
        pltpu.make_async_copy(filter_keys_h, filter_keys, load_sem.at[16]),
        pltpu.make_async_copy(filter_query_h, filter_query, load_sem.at[17]),
        pltpu.make_async_copy(sink_h, sink, load_sem.at[18]),
        pltpu.make_async_copy(out_state_w, wout.at[me, pl.ds(0, LANES), :], load_sem.at[7]),
        pltpu.make_async_copy(
            out_window_w, wout.at[me, pl.ds(LANES, 2 * LANES), :], load_sem.at[8]
        ),
    ]
    for load in loads + late_loads:
        load.start()

    barrier = pltpu.get_barrier_semaphore()
    peers = [{"sp": modulo(me + o, n)} for o in sorted({1, n - 1})]
    peers += [{"fs": modulo(my_y + o, ny)} for o in sorted({1, ny - 1})]
    peers += [{"tp": partner}]
    peers += [{"tp": 2 * modulo(my_x + o, nx) + core} for o in sorted({1, nx - 1}) if nx > 1]
    for peer in peers:
        pl.semaphore_signal(barrier, inc=1, device_id=peer)
    for load in loads:
        load.wait()
    pl.semaphore_wait(barrier, len(peers))

    def halo_copy(d):
        source = tokens.at[pl.ds(rows - HALO, HALO)] if d == 0 else tokens.at[pl.ds(0, HALO)]
        return pltpu.make_async_remote_copy(
            source,
            halo_in.at[d],
            hs.at[d],
            hr.at[d],
            device_id={"sp": right if d == 0 else left},
        )

    buffers = (win, wout)
    pieces = (PIECES, 2)
    z_sems = ((zs, zr), (czs, czr))
    y_sems = ((ys, yr), (cys, cyr))

    def slab(k, source, which, q):
        size = buffers[k].shape[1] // (2 * pieces[k])
        start = pl.multiple_of((pieces[k] * which + q) * size, size)
        return buffers[k].at[source, pl.ds(start, size)]

    def lower(k, q):
        return q < pieces[k] // 2

    def origin(d, s):
        return modulo(me - s, n) if d == 0 else modulo(me + s, n)

    def z_move(d, s, k, q, source):
        ref = slab(k, source, own_half, q)
        sent, landed = z_sems[k]
        return pltpu.make_async_remote_copy(
            ref,
            ref,
            sent.at[d, s - 1, q],
            landed.at[d, s - 1, q],
            device_id={"sp": right if d == 0 else left},
        )

    def z_copy(d, s, k, q):
        return z_move(d, s, k, q, origin(d, s - 1))

    def z_arrival(d, s, k, q):
        return z_move(d, s, k, q, origin(d, s))

    def y_copy(d, s, k, q, which):
        ref = slab(k, origin(d, s), which, q)
        sent, landed = y_sems[k]
        return pltpu.make_async_remote_copy(
            ref,
            ref,
            sent.at[d, s - 1, q],
            landed.at[d, s - 1, q],
            device_id={"fs": up if lower(k, q) else down},
        )

    def last_way(k, q, d):
        return lower(k, q) == (d == 0)

    def set_off(k):
        for q in range(pieces[k]):
            for d in range(2):
                if half > 1 or last_way(k, q, d):
                    z_copy(d, 1, k, q).start()

    def relay(k, s):
        @pl.when(s < half)
        def _():
            for q in range(pieces[k]):
                for d in range(2):
                    z_arrival(d, s, k, q).wait_recv()
                    if last_way(k, q, d):
                        z_copy(d, s + 1, k, q).start()
                    else:

                        @pl.when(s + 1 < half)
                        def _():
                            z_copy(d, s + 1, k, q).start()

                    y_copy(d, s, k, q, own_half).start()

        @pl.when(s == half)
        def _():
            for q in range(pieces[k]):
                for d in range(2):
                    if last_way(k, q, d):
                        z_arrival(d, s, k, q).wait_recv()
                        y_copy(d, s, k, q, own_half).start()

    def y_landed(k, s):
        @pl.when((s >= 1) & (s < half))
        def _():
            for q in range(pieces[k]):
                for d in range(2):
                    y_copy(d, s, k, q, 1 - own_half).wait_recv()

        @pl.when(s == half)
        def _():
            for q in range(pieces[k]):
                for d in range(2):
                    if last_way(k, q, d):
                        y_copy(d, s, k, q, 1 - own_half).wait_recv()

    set_off(0)
    for load in late_loads:
        load.wait()
    for d in range(2):
        halo_copy(d).start()

    def normalise(x):
        wide = x.astype(F32)
        scale = lax.rsqrt(jnp.mean(wide * wide, axis=-1, keepdims=True) + 1e-06)
        return (wide * scale * norm_gain[...]).astype(BF16)

    def normalise_chunk(i, carry):
        start = pl.multiple_of(i * 32, 32)
        normed[pl.ds(HALO + start, 32), :] = normalise(tokens[pl.ds(start, 32), :])
        return carry

    lax.fori_loop(0, rows // 64, normalise_chunk, 0)
    if half > 1:
        relay(0, 1)
    lax.fori_loop(rows // 64, rows // 32, normalise_chunk, 0)
    for d in range(2):
        halo_copy(d).wait_recv()
        normed[(0 if d == 0 else HALO + rows) : (HALO if d == 0 else 2 * HALO + rows), :] = (
            normalise(halo_in[d])
        )

    def slice_of(source):
        return normed[:, pl.ds(pl.multiple_of(source * shard, shard), shard)]

    def project(sources, first):
        for c in range(0, WIN_COLS, 256):
            term = functools.reduce(
                jnp.add, [dot(slice_of(o), win[o, :, c : c + 256]) for o in sources]
            )
            if first:
                acc[:, c : c + 256] = term
            else:
                acc[:, c : c + 256] += term

    heads = lax.broadcasted_iota(jnp.int32, (LANES, step_w.shape[0]), 1)
    lanes_of = lax.broadcasted_iota(jnp.int32, (LANES, step_w.shape[0]), 0)
    spread = (heads == 2 * my_tp + lanes_of // (LANES // 2)).astype(BF16)
    step_cols[...] = dot(spread, step_w[...]).astype(BF16)
    tri = (
        lax.broadcasted_iota(jnp.int32, (BLOCK, BLOCK), 0)
        >= lax.broadcasted_iota(jnp.int32, (BLOCK, BLOCK), 1)
    ).astype(F32)
    first_head = half_lanes((1, LANES))
    first_rows = lax.broadcasted_iota(jnp.int32, (LANES, BLOCK), 0) < LANES // 2

    def decay_block(b):
        start = pl.multiple_of(b * BLOCK, BLOCK)
        raw = lax.dot_general(
            normed[pl.ds(HALO + start, BLOCK), :],
            step_cols[...],
            (((1,), (1,)), ((), ())),
            preferred_element_type=F32,
        )
        step = jnp.maximum(raw, 0.0) + jnp.log1p(jnp.exp(-jnp.abs(raw)))
        rate_row = jnp.where(first_head, rate[:, 0:1], rate[:, 1:2])
        jump = jumps[:, pl.ds(start, BLOCK)]
        logs = -rate_row * step + jnp.where(first_rows, jump[0:1, :], jump[1:2, :]).T
        step_b[pl.ds(start, BLOCK), :] = step
        cum_b[pl.ds(start, BLOCK), :] = dot(tri, logs, HIGHEST)

    angle_rows = rows // half

    def angle_block(i):
        start = pl.multiple_of(i * angle_rows, angle_rows)
        lane = lax.broadcasted_iota(jnp.int32, (angle_rows, LANES), 1)
        position = (
            lax.broadcasted_iota(jnp.int32, (angle_rows, LANES), 0) + me * rows + start
        )
        row_at = (position // GRID_WIDTH).astype(F32)
        col_at = lax.rem(position, GRID_WIDTH).astype(F32)
        exponent = lax.rem(lane, QUARTER).astype(F32) / -QUARTER
        inverse = jnp.exp(exponent[0:8] * 9.210340371976184)[0:1]
        angle = jnp.where(lane < LANES // 2, row_at, col_at) * inverse
        sine = jnp.sin(angle)
        cos_t[pl.ds(start, angle_rows), :] = jnp.cos(angle)
        sin_t[pl.ds(start, angle_rows), :] = jnp.where(
            lax.rem(lane, 2 * QUARTER) < QUARTER, -sine, sine
        )

    def gather_step(s, carry):
        @pl.when(s > 1)
        def _():
            relay(0, s)

        @pl.when(s == 1)
        def _():
            if half == 1:
                relay(0, s)
            project([me], True)

        @pl.when(s == out_lag)
        def _():
            set_off(1)

        @pl.when(s > out_lag)
        def _():
            relay(1, s - out_lag)

        @pl.when(s <= half)
        def _():
            angle_block(s - 1)

        @pl.when(s <= blocks)
        def _():
            decay_block(s - 1)

        before = s - 1
        y_landed(0, before)

        @pl.when((before >= 1) & (before < half))
        def _():
            project([origin(0, before), origin(1, before)], False)

        @pl.when(before == half)
        def _():
            project([origin(0, before)], False)

        return carry

    out_lag = max(half + 1 - OUT_EARLY, 1)
    lax.fori_loop(1, half + 2, gather_step, 0)
    for b in range(half + 1, blocks):
        decay_block(b)

    def rotate(x, b):
        start = pl.multiple_of(b * BLOCK, BLOCK)
        wide = x.astype(BF16).astype(F32)
        lane = lax.broadcasted_iota(jnp.int32, (BLOCK, LANES), 1)
        turned = jnp.where(
            lax.rem(lane, 2 * QUARTER) < QUARTER,
            pltpu.roll(wide, LANES - QUARTER, 1),
            pltpu.roll(wide, QUARTER, 1),
        )
        return (
            wide * cos_t[pl.ds(start, BLOCK), :] + turned * sin_t[pl.ds(start, BLOCK), :]
        ).astype(BF16)

    def key_block(b, carry):
        start = pl.multiple_of(b * BLOCK, BLOCK)
        own = pl.ds(HALO + start, BLOCK)
        target = pl.ds(BLOCK + start, BLOCK)
        kv_ext[target, 0:LANES] = rotate(acc[own, 768:896], b)
        kv_ext[target, LANES : 2 * LANES] = acc[own, 896:1024].astype(BF16)
        return carry

    def query_block(b, carry):
        start = pl.multiple_of(b * BLOCK, BLOCK)
        own = pl.ds(HALO + start, BLOCK)
        for h in range(2):
            query_rot[pl.ds(start, BLOCK), h * LANES : (h + 1) * LANES] = rotate(
                acc[own, 512 + h * LANES : 512 + (h + 1) * LANES], b
            )
        return carry

    lax.fori_loop(0, blocks, key_block, 0)

    def kv_copy(d):
        source = kv_ext.at[pl.ds(rows if d == 0 else BLOCK, BLOCK)]
        return pltpu.make_async_remote_copy(
            source,
            kv_ext.at[pl.ds(0 if d == 0 else rows + BLOCK, BLOCK)],
            ks.at[d],
            kr.at[d],
            device_id={"sp": right if d == 0 else left},
        )

    pre[...] = acc[:, 0:384].astype(BF16).astype(F32)

    @pl.when(me == 0)
    def _():
        pre[0:HALO, :] = jnp.zeros((HALO, 384), F32)

    @pl.when(me == n - 1)
    def _():
        pre[HALO + rows : 2 * HALO + rows, :] = jnp.zeros((HALO, 384), F32)

    for d in range(2):
        kv_copy(d).start()

    taps = [f[...].astype(F32) for f in (filter_value, filter_keys, filter_query)]
    for b in range(blocks):
        for c in range(3):
            total = jnp.zeros((BLOCK, LANES), F32)
            for j in range(5):
                at = HALO + b * BLOCK + j - 2
                total = total + (
                    pre[at : at + BLOCK, c * LANES : (c + 1) * LANES] * taps[c][j : j + 1, :]
                )
            here = slice(b * BLOCK, (b + 1) * BLOCK)
            if c == 0:
                scan_v[here, :] = total * jax.nn.sigmoid(total) * step_b[here, :]
            elif c == 1:
                scan_k[here, :] = total.astype(BF16)
            else:
                scan_q[here, :] = total.astype(BF16)

    def block_states(b, carry):
        start = pl.multiple_of(b * BLOCK, BLOCK)
        here = pl.ds(start, BLOCK)
        cum = cum_b[here, :]
        total = cum[BLOCK - 1 : BLOCK, :]
        values = scan_v[here, :].astype(BF16).astype(F32)
        keys_t = scan_k[here, :].astype(F32).T.astype(BF16)
        state_a[b] = dot(keys_t, (values * jnp.exp(total - cum)).astype(BF16))
        state_c[b] = dot(keys_t, (values * jnp.exp(cum)).astype(BF16))
        return carry

    lax.fori_loop(0, blocks, block_states, 0)
    ends = [cum_b[(b + 1) * BLOCK - 1 : (b + 1) * BLOCK, :] for b in range(blocks)]
    forward = jnp.zeros((BLOCK, LANES), F32)
    for b in range(blocks):
        carry_f[b] = forward.astype(BF16)
        forward = forward * jnp.exp(ends[b]) + state_a[b]
    backward = jnp.zeros((BLOCK, LANES), F32)
    for b in reversed(range(blocks)):
        carry_b[b] = backward.astype(BF16)
        backward = backward * jnp.exp(ends[b]) + state_c[b]
    overall = functools.reduce(jnp.add, ends)

    piece = BLOCK // n
    message[...] = jnp.concatenate(
        [forward.reshape(n, piece, LANES), backward.reshape(n, piece, LANES)], axis=1
    ).astype(BF16)
    totals_out[...] = overall
    totals[me] = overall
    arrived[me] = message[me]

    def first_exchange(o):
        to = modulo(me + o, n)
        return (
            pltpu.make_async_remote_copy(
                message.at[to], arrived.at[me], a1s.at[o], a1r.at[o], device_id={"sp": to}
            ),
            pltpu.make_async_remote_copy(
                totals_out, totals.at[me], ts.at[o], tr.at[o], device_id={"sp": to}
            ),
        )

    def first_arrival(o):
        source = modulo(me - o, n)
        return (
            pltpu.make_async_remote_copy(
                arrived.at[source], arrived.at[source], a1s.at[o], a1r.at[o], device_id={"sp": source}
            ),
            pltpu.make_async_remote_copy(
                totals.at[source], totals.at[source], ts.at[o], tr.at[o], device_id={"sp": source}
            ),
        )

    order = sorted(range(1, n), key=lambda o: -min(o, n - o))
    for o in order:
        for copy in first_exchange(o):
            copy.start()

    out_next = [half + 2 - out_lag]

    def serve_out(last=False):
        while out_next[0] <= half:
            relay(1, out_next[0])
            out_next[0] += 1
            if not last:
                break

    serve_out()

    near_mask = half_lanes((BLOCK, LANES))

    def local_scan(b, carry):
        start = pl.multiple_of(b * BLOCK, BLOCK)
        here = pl.ds(start, BLOCK)
        cum = cum_b[here, :]
        cum_t = cum.T
        total = cum[BLOCK - 1 : BLOCK, :]
        values = scan_v[here, :].astype(BF16)
        query = scan_q[here, :]
        gram = lax.dot_general(
            query, scan_k[here, :], (((1,), (1,)), ((), ())), preferred_element_type=F32
        )
        near = []
        for h in range(2):
            lane = h * (LANES // 2)
            gap = jnp.abs(cum[:, lane : lane + 1] - cum_t[lane : lane + 1, :])
            near.append(dot((gram * jnp.exp(-gap)).astype(BF16), values))
        out = jnp.where(near_mask, near[0], near[1])
        out += jnp.exp(cum) * dot(query, carry_f[b])
        out += jnp.exp(total - cum) * dot(query, carry_b[b])
        scan_loc[here, :] = out
        return carry

    lax.fori_loop(0, blocks, local_scan, 0)

    serve_out()

    lax.fori_loop(0, blocks, query_block, 0)
    for d in range(2):
        kv_copy(d).wait_recv()

    def attend(b, carry):
        start = pl.multiple_of(b * BLOCK, BLOCK)
        band = kv_ext[pl.ds(start, 3 * BLOCK), :]
        row = lax.broadcasted_iota(jnp.int32, (BLOCK, 3 * BLOCK), 0)
        col = lax.broadcasted_iota(jnp.int32, (BLOCK, 3 * BLOCK), 1)
        where_key = me * rows - BLOCK + start + col
        valid = (
            (jnp.abs(col - BLOCK - row) <= BLOCK) & (where_key >= 0) & (where_key < n * rows)
        )
        for h in range(2):
            query = query_rot[pl.ds(start, BLOCK), h * LANES : (h + 1) * LANES]
            scores = lax.dot_general(
                query, band[:, 0:LANES], (((1,), (1,)), ((), ())), preferred_element_type=F32
            ) * LANES ** (-0.5)
            masked = jnp.where(valid, scores, -1e30)
            ceiling = jnp.maximum(jnp.max(masked, axis=-1, keepdims=True), sink[:, h : h + 1])
            weights = jnp.where(valid, jnp.exp(masked - ceiling), 0.0)
            bottom = jnp.exp(sink[:, h : h + 1] - ceiling) + jnp.sum(weights, axis=-1, keepdims=True)
            probs = (weights / bottom).astype(BF16)
            mix[pl.ds(start, BLOCK), (1 + h) * LANES : (2 + h) * LANES] = dot(
                probs, band[:, LANES : 2 * LANES]
            ).astype(BF16)
        return carry

    lax.fori_loop(0, blocks // 2, attend, 0)
    serve_out()

    for o in order:
        for copy in first_arrival(o):
            copy.wait_recv()

    running = jnp.zeros((piece, LANES), F32)
    ahead = []
    for d in range(n):
        ahead.append(running)
        running = running * jnp.exp(totals[d]) + arrived[d].astype(F32)[0:piece]
    running = jnp.zeros((piece, LANES), F32)
    behind = [None] * n
    for d in reversed(range(n)):
        behind[d] = running
        running = running * jnp.exp(totals[d]) + arrived[d].astype(F32)[piece : 2 * piece]
    for d in range(n):
        income_out[d] = jnp.concatenate([ahead[d], behind[d]], axis=0).astype(BF16)
    incoming[me] = income_out[me]

    def second_exchange(o):
        to = modulo(me + o, n)
        return pltpu.make_async_remote_copy(
            income_out.at[to], incoming.at[me], a2s.at[o], a2r.at[o], device_id={"sp": to}
        )

    def second_arrival(o):
        source = modulo(me - o, n)
        return pltpu.make_async_remote_copy(
            incoming.at[source], incoming.at[source], a2s.at[o], a2r.at[o], device_id={"sp": source}
        )

    for o in order:
        second_exchange(o).start()

    serve_out()
    lax.fori_loop(blocks // 2, blocks, attend, 0)
    serve_out(True)

    def wait_out(s, carry):
        y_landed(1, s)
        return carry

    lax.fori_loop(1, half + 1, wait_out, 0)

    def out_weights(i, low, size):
        return jnp.concatenate(
            [wout[2 * i, low : low + size, :], wout[2 * i + 1, low : low + size, :]], axis=1
        )

    def window_product(i, carry):
        columns = pl.ds(pl.multiple_of(i * 2 * LANES, 2 * LANES), 2 * LANES)
        part_sum[:, columns] = dot(mix[:, LANES:], out_weights(i, LANES, 2 * LANES))
        return carry

    lax.fori_loop(0, n // 2, window_product, 0)

    for o in order:
        second_arrival(o).wait_recv()
    incomes = incoming[...].astype(F32)
    income_f = incomes[:, 0:piece].reshape(BLOCK, LANES).astype(BF16)
    income_b = incomes[:, piece : 2 * piece].reshape(BLOCK, LANES).astype(BF16)
    befores = [jnp.zeros((1, LANES), F32)]
    for b in range(blocks):
        befores.append(befores[-1] + ends[b])
    for b in range(blocks):
        here = slice(b * BLOCK, (b + 1) * BLOCK)
        cum = cum_b[here, :]
        query = scan_q[here, :]
        after = overall - befores[b + 1]
        out = scan_loc[here, :]
        out += jnp.exp(cum + befores[b]) * dot(query, income_f)
        out += jnp.exp(ends[b] - cum + after) * dot(query, income_b)
        gate = acc[HALO + b * BLOCK : HALO + (b + 1) * BLOCK, 384:512].astype(BF16).astype(F32)
        gated = out * (gate * jax.nn.sigmoid(gate))
        square = gated * gated
        low = jnp.sum(jnp.where(near_mask, square, 0.0), axis=-1, keepdims=True)
        high = jnp.sum(jnp.where(near_mask, 0.0, square), axis=-1, keepdims=True)
        mean = jnp.where(near_mask, low, high) * (2.0 / LANES)
        mix[here, 0:LANES] = (gated * lax.rsqrt(mean + 1e-06) * gain[...]).astype(BF16)

    unit = rows // (2 * nx)

    def group_product(x):
        first = pl.multiple_of(x * 2 * unit, 2 * unit)
        theirs = pl.multiple_of((1 - core) * unit, unit)
        lhs = mix[pl.ds(first, 2 * unit), 0:LANES]

        def tile(i, carry):
            columns = pl.ds(pl.multiple_of(i * 2 * LANES, 2 * LANES), 2 * LANES)
            part_sum[pl.ds(first, 2 * unit), columns] += dot(lhs, out_weights(i, 0, LANES))
            pair_out[x, :, columns] = part_sum[pl.ds(first + theirs, unit), columns].astype(BF16)
            return carry

        lax.fori_loop(0, n // 2, tile, 0)

    def pair_copy(x):
        return pltpu.make_async_remote_copy(
            pair_out.at[x], pair_in.at[x], ps.at[x], pr.at[x], device_id={"tp": partner}
        )

    x_order = sorted(range(nx), key=lambda o: -min(o, nx - o))
    groups = [modulo(my_x + o, nx) for o in x_order]
    for x in groups:
        group_product(x)
        pair_copy(x).start()

    side = unit // 2

    def group_sum(x, h):
        first = pl.multiple_of((2 * x + core) * unit + h * side, side)
        return part_sum[pl.ds(first, side), :] + pair_in[x, h * side : (h + 1) * side, :].astype(
            F32
        )

    next_x, last_x = modulo(my_x + 1, nx), modulo(my_x - 1, nx)

    def x_copy(i, source, target, d):
        return pltpu.make_async_remote_copy(
            source.at[d],
            target.at[d],
            gs.at[i, d],
            gr.at[i, d],
            device_id={"tp": 2 * (next_x if d == 0 else last_x) + core},
        )

    def via(d):
        return x_copy(0, via_out, via_in, d)

    def direct(d):
        return x_copy(1, direct_out, direct_in, d)

    def merged(d):
        return x_copy(2, merged_out, merged_in, d)

    beside = (next_x, last_x)
    if nx == 4:
        far = modulo(my_x + 2, nx)
        pair_copy(far).wait_recv()
        for d in range(2):
            via_out[d] = group_sum(far, d).astype(BF16)
            via(d).start()
    if nx > 1:
        for x in sorted({0, 1} if nx > 2 else {0}):
            pair_copy(beside[x]).wait_recv()
        for d in range(2):
            direct_out[d] = group_sum(beside[d], 1 - d).astype(BF16)
            direct(d).start()
    if nx == 4:
        for d in range(2):
            via(d).wait_recv()
            merged_out[d] = (group_sum(beside[d], d) + via_in[d].astype(F32)).astype(BF16)
            merged(d).start()
    pair_copy(my_x).wait_recv()
    for h in range(2):
        mine = group_sum(my_x, h)
        if nx > 1:
            direct(1 - h).wait_recv()
            mine = mine + direct_in[1 - h].astype(F32)
        if nx == 4:
            merged(h).wait_recv()
            mine = mine + merged_in[h].astype(F32)
        result[h * side : (h + 1) * side, :] = mine.astype(BF16)

    for d in range(2):
        halo_copy(d).wait_send()
        kv_copy(d).wait_send()
    for o in order:
        for copy in first_exchange(o):
            copy.wait_send()
        second_exchange(o).wait_send()
    for x in range(nx):
        pair_copy(x).wait_send()
    for d in range(2):
        if nx == 4:
            via(d).wait_send()
            merged(d).wait_send()
        if nx > 1:
            direct(d).wait_send()

    def drain(s, carry):
        for k in range(2):
            for q in range(pieces[k]):
                for d in range(2):
                    if last_way(k, q, d):
                        z_copy(d, s, k, q).wait_send()
                        y_copy(d, s, k, q, own_half).wait_send()
                    else:

                        @pl.when(s < half)
                        def _():
                            z_copy(d, s, k, q).wait_send()
                            y_copy(d, s, k, q, own_half).wait_send()

        return carry

    lax.fori_loop(1, half + 1, drain, 0)


def solution(mesh):
    n, ny, nt = (mesh.shape[a] for a in ("sp", "fs", "tp"))
    nx = nt // 2

    def shards(*args):
        args = list(args)
        rows, depth = args[0].shape
        for i in (1, 7, 9, 16):
            args[i] = args[i].reshape(1, -1)
        for i in (6, 8):
            args[i] = args[i].T
        shard = depth // n
        half = n // 2
        blocks = rows // BLOCK
        piece = BLOCK // n
        unit = rows // (2 * nx)
        vmem = pl.BlockSpec(memory_space=pltpu.VMEM)
        specs = [pl.BlockSpec(memory_space=pl.ANY)] * 19
        dma = pltpu.SemaphoreType.DMA
        V = pltpu.VMEM
        kept = (0, 1, 6, 7, 8, 9, 10, 11, 12, 16)
        scratch = [V(args[i].shape, args[i].dtype) for i in kept]
        scratch += [
            V((n, shard, WIN_COLS), BF16),
            V((n, 3 * LANES, LANES), BF16),
            V((rows + 2 * HALO, depth), BF16),
            V((rows + 2 * HALO, WIN_COLS), F32),
            V((2, HALO, depth), BF16),
            V((rows + 2 * HALO, 3 * LANES), F32),
            V((rows, LANES), F32),
            V((rows, LANES), F32),
            V((rows, LANES), F32),
            V((rows, LANES), F32),
            V((LANES, depth), BF16),
            V((rows, LANES), F32),
            V((rows, LANES), BF16),
            V((rows, LANES), BF16),
            V((rows, 2 * LANES), BF16),
            V((rows + 2 * BLOCK, 2 * LANES), BF16),
            V((blocks, BLOCK, LANES), F32),
            V((blocks, BLOCK, LANES), F32),
            V((blocks, BLOCK, LANES), BF16),
            V((blocks, BLOCK, LANES), BF16),
            V((rows, LANES), F32),
            V((n, 2 * piece, LANES), BF16),
            V((n, 2 * piece, LANES), BF16),
            V((1, LANES), F32),
            V((n, 1, LANES), F32),
            V((n, 2 * piece, LANES), BF16),
            V((n, 2 * piece, LANES), BF16),
            V((rows, 3 * LANES), BF16),
            V((rows, depth), F32),
            V((nx, unit, depth), BF16),
            V((nx, unit, depth), BF16),
            *[V((2, unit // 2, depth), BF16)] * 6,
            dma((19,)),
            *[dma((2, half, PIECES))] * 4,
            *[dma((2, half, 2))] * 4,
            dma((2,)),
            dma((2,)),
            dma((2,)),
            dma((2,)),
            dma((n,)),
            dma((n,)),
            dma((n,)),
            dma((n,)),
            dma((n,)),
            dma((n,)),
            dma((nx,)),
            dma((nx,)),
            dma((3, 2)),
            dma((3, 2)),
        ]
        return pl.pallas_call(
            functools.partial(kernel, n, ny, nx),
            out_shape=jax.ShapeDtypeStruct((rows // nt, depth), BF16),
            in_specs=specs,
            out_specs=vmem,
            scratch_shapes=scratch,
            compiler_params=pltpu.CompilerParams(
                collective_id=0, has_side_effects=True, vmem_limit_bytes=60 * 1024 * 1024
            ),
        )(*args)

    placed = (
        P(("fs", "sp"), None),
        P(),
        P("sp", "tp"),
        P("sp", "tp"),
        P("sp", "tp"),
        P("sp", "tp"),
        P(),
        P("tp"),
        P(("fs", "sp"), "tp"),
        P("tp"),
        P(None, "tp"),
        P(None, "tp"),
        P(None, "tp"),
        P("sp", "tp"),
        P("sp", "tp"),
        P("sp", "tp"),
        P("tp"),
        P("tp", "sp"),
        P("tp", "sp"),
    )
    return jax.shard_map(
        shards, mesh=mesh, in_specs=placed, out_specs=P(("fs", "sp", "tp"), None), check_vma=False
    )
```

```python
import functools

import jax
import jax.numpy as jnp
from jax import lax
from jax.experimental import pallas as pl
from jax.experimental.pallas import tpu as pltpu
from jax.sharding import PartitionSpec as P

BLOCK = 128
LANES = 128
HALO = 16
GRID_WIDTH = 64
QUARTER = 32
WIN_COLS = 1024
PIECES = 2
TILE = 256
OUT_LAG = 4
F32 = jnp.float32
BF16 = jnp.bfloat16
HIGHEST = lax.Precision.HIGHEST


def modulo(value, count):
    return lax.rem(value + 2 * count, count)


def half_lanes(shape):
    return lax.broadcasted_iota(jnp.int32, shape, 1) < LANES // 2


def dot(a, b, precision=None):
    return jnp.dot(a, b, preferred_element_type=F32, precision=precision)


def kernel(
    n,
    ny,
    nx,
    tokens_h,
    norm_gain_h,
    gate_w,
    value_w,
    keys_w,
    query_w,
    step_h,
    rate_h,
    jumps_h,
    gain_h,
    filter_value_h,
    filter_keys_h,
    filter_query_h,
    wq_w,
    wk_w,
    wv_w,
    sink_h,
    out_state_w,
    out_window_w,
    result,
    tokens,
    norm_gain,
    step_w,
    rate,
    jumps,
    gain,
    filter_value,
    filter_keys,
    filter_query,
    sink,
    win,
    wout,
    pwin,
    pwout,
    normed,
    acc,
    halo_in,
    pre,
    cos_t,
    sin_t,
    step_b,
    cum_b,
    step_cols,
    scan_v,
    scan_k,
    scan_q,
    query_rot,
    kv_ext,
    state_a,
    state_c,
    carry_f,
    carry_b,
    scan_loc,
    message,
    arrived,
    totals_out,
    totals,
    incoming,
    income_out,
    mix,
    part_sum,
    pair_out,
    pair_in,
    via_out,
    via_in,
    direct_out,
    direct_in,
    merged_out,
    merged_in,
    load_sem,
    zs,
    zr,
    ys,
    yr,
    czs,
    czr,
    cys,
    cyr,
    pzs,
    pzr,
    pys,
    ds,
    dr,
    cpzs,
    cpzr,
    cpys,
    cds,
    cdr,
    hs,
    hr,
    ks,
    kr,
    a1s,
    a1r,
    a2s,
    a2r,
    ts,
    tr,
    ps,
    pr,
    gs,
    gr,
):
    rows = tokens.shape[0]
    blocks = rows // BLOCK
    depth = tokens.shape[1]
    shard = depth // n
    me = lax.axis_index("sp")
    my_y = lax.axis_index("fs")
    my_tp = lax.axis_index("tp")
    core = lax.rem(my_tp, 2)
    my_x = my_tp // 2
    right, left = modulo(me + 1, n), modulo(me - 1, n)
    up, down = modulo(my_y + 1, ny), modulo(my_y - 1, ny)
    partner = my_tp + 1 - 2 * core
    own_half = lax.rem(my_y, 2)
    half = n // 2

    loads = []
    column = 0
    for k, ref in enumerate((value_w, keys_w, query_w, gate_w, wq_w, wk_w, wv_w)):
        width = ref.shape[1]
        loads.append(
            pltpu.make_async_copy(ref, win.at[me, :, pl.ds(column, width)], load_sem.at[k])
        )
        column += width
    late_loads = [
        pltpu.make_async_copy(tokens_h, tokens, load_sem.at[9]),
        pltpu.make_async_copy(norm_gain_h, norm_gain, load_sem.at[10]),
        pltpu.make_async_copy(step_h, step_w, load_sem.at[11]),
        pltpu.make_async_copy(rate_h, rate, load_sem.at[12]),
        pltpu.make_async_copy(jumps_h, jumps, load_sem.at[13]),
        pltpu.make_async_copy(gain_h, gain, load_sem.at[14]),
        pltpu.make_async_copy(filter_value_h, filter_value, load_sem.at[15]),
        pltpu.make_async_copy(filter_keys_h, filter_keys, load_sem.at[16]),
        pltpu.make_async_copy(filter_query_h, filter_query, load_sem.at[17]),
        pltpu.make_async_copy(sink_h, sink, load_sem.at[18]),
        pltpu.make_async_copy(out_state_w, wout.at[me, pl.ds(0, LANES), :], load_sem.at[7]),
        pltpu.make_async_copy(
            out_window_w, wout.at[me, pl.ds(LANES, 2 * LANES), :], load_sem.at[8]
        ),
    ]
    for load in loads + late_loads:
        load.start()

    barrier = pltpu.get_barrier_semaphore()
    both = (my_tp, partner)
    peers = [{"sp": modulo(me + o, n), "tp": t} for o in sorted({1, n - 1}) for t in both]
    peers += [{"fs": modulo(my_y + o, ny), "tp": t} for o in sorted({1, ny - 1}) for t in both]
    peers += [{"tp": partner}]
    peers += [{"tp": 2 * modulo(my_x + o, nx) + core} for o in sorted({1, nx - 1}) if nx > 1]
    for peer in peers:
        pl.semaphore_signal(barrier, inc=1, device_id=peer)
    for load in loads:
        load.wait()
    pl.semaphore_wait(barrier, len(peers))

    def halo_copy(d):
        source = tokens.at[pl.ds(rows - HALO, HALO)] if d == 0 else tokens.at[pl.ds(0, HALO)]
        return pltpu.make_async_remote_copy(
            source,
            halo_in.at[d],
            hs.at[d],
            hr.at[d],
            device_id={"sp": right if d == 0 else left},
        )

    relays = core == 1
    buffers = (win, wout)
    passing = (pwin, pwout)
    pieces = (PIECES, 2)
    p_sems = ((pzs, pzr, pys, ds, dr, yr), (cpzs, cpzr, cpys, cds, cdr, cyr))
    z_sems = ((zs, zr), (czs, czr))
    y_sems = ((ys, yr), (cys, cyr))

    def slab(k, source, which, q):
        size = buffers[k].shape[1] // (2 * pieces[k])
        start = pl.multiple_of((pieces[k] * which + q) * size, size)
        return buffers[k].at[source, pl.ds(start, size)]

    def lower(k, q):
        return q < pieces[k] // 2

    def origin(d, s):
        return modulo(me - s, n) if d == 0 else modulo(me + s, n)

    def z_move(d, s, k, q, source):
        ref = slab(k, source, own_half, q)
        sent, landed = z_sems[k]
        return pltpu.make_async_remote_copy(
            ref,
            ref,
            sent.at[d, s - 1, q],
            landed.at[d, s - 1, q],
            device_id={"sp": right if d == 0 else left},
        )

    def z_copy(d, s, k, q):
        return z_move(d, s, k, q, origin(d, s - 1))

    def z_arrival(d, s, k, q):
        return z_move(d, s, k, q, origin(d, s))

    def y_copy(d, s, k, q, which):
        ref = slab(k, origin(d, s), which, q)
        sent, landed = y_sems[k]
        return pltpu.make_async_remote_copy(
            ref,
            ref,
            sent.at[d, s - 1, q],
            landed.at[d, s - 1, q],
            device_id={"fs": up if lower(k, q) else down},
        )

    def last_way(k, q, d):
        return lower(k, q) == (d == 0)

    def p_slab(k, source, q):
        size = buffers[k].shape[1] // (2 * pieces[k])
        return passing[k].at[source, pl.ds(q * size, size)]

    def along(d):
        return right if d == 0 else left

    def p_first(d, k, q):
        return pltpu.make_async_remote_copy(
            slab(k, me, own_half, q),
            p_slab(k, me, q),
            p_sems[k][0].at[d, 0, q],
            p_sems[k][1].at[d, 0, q],
            device_id={"sp": along(d), "tp": partner},
        )

    def p_move(d, s, k, q, source):
        ref = p_slab(k, source, q)
        return pltpu.make_async_remote_copy(
            ref,
            ref,
            p_sems[k][0].at[d, s - 1, q],
            p_sems[k][1].at[d, s - 1, q],
            device_id={"sp": along(d)},
        )

    def p_copy(d, s, k, q):
        return p_move(d, s, k, q, origin(d, s - 1))

    def p_arrival(d, s, k, q):
        return p_move(d, s, k, q, origin(d, s))

    def p_side(d, s, k, q):
        source = origin(d, s)
        return pltpu.make_async_remote_copy(
            p_slab(k, source, q),
            slab(k, source, own_half, q),
            p_sems[k][2].at[d, s - 1, q],
            p_sems[k][5].at[d, s - 1, q],
            device_id={"fs": up if lower(k, q) else down, "tp": partner},
        )

    def p_down(d, s, k, q):
        source = origin(d, s)
        return pltpu.make_async_remote_copy(
            p_slab(k, source, q),
            slab(k, source, own_half, q),
            p_sems[k][3].at[d, s - 1, q],
            p_sems[k][4].at[d, s - 1, q],
            device_id={"tp": partner},
        )

    def first_pieces(k):
        return [
            (d, q)
            for q in range(pieces[k])
            for d in range(2)
            if half > 1 or last_way(k, q, d)
        ]

    def set_off(k):
        @pl.when(relays)
        def _():
            for d, q in first_pieces(k):
                z_copy(d, 1, k, q).start()

        @pl.when(jnp.logical_not(relays))
        def _():
            for d, q in first_pieces(k):
                p_first(d, k, q).start()

    def pass_on(k, s, q, d):
        for arrival, onward, others in (
            (z_arrival, z_copy, (lambda *at: y_copy(*at, own_half),)),
            (p_arrival, p_copy, (p_side, p_down)),
        ):
            arrival(d, s, k, q).wait_recv()
            if last_way(k, q, d):

                @pl.when(s < half)
                def _():
                    onward(d, s + 1, k, q).start()
            else:

                @pl.when(s + 1 < half)
                def _():
                    onward(d, s + 1, k, q).start()

            for other in others:
                other(d, s, k, q).start()

    def relay_piece(k, s, q):
        @pl.when(relays & (s >= 1) & (s <= half))
        def _():
            for d in range(2):
                if last_way(k, q, d):
                    pass_on(k, s, q, d)
                else:

                    @pl.when(s < half)
                    def _():
                        pass_on(k, s, q, d)

    def relay(k, s):
        for q in range(pieces[k]):
            relay_piece(k, s, q)

    def y_landed(k, s):
        def landed(d, q):
            y_copy(d, s, k, q, 1 - own_half).wait_recv()

            @pl.when(jnp.logical_not(relays))
            def _():
                p_down(d, s, k, q).wait_recv()

        @pl.when((s >= 1) & (s <= half))
        def _():
            for q in range(pieces[k]):
                for d in range(2):
                    if last_way(k, q, d):
                        landed(d, q)
                    else:

                        @pl.when(s < half)
                        def _():
                            landed(d, q)

    set_off(0)
    for load in late_loads:
        load.wait()
    for d in range(2):
        halo_copy(d).start()

    def normalise(x):
        wide = x.astype(F32)
        scale = lax.rsqrt(jnp.mean(wide * wide, axis=-1, keepdims=True) + 1e-06)
        return (wide * scale * norm_gain[...]).astype(BF16)

    def normalise_chunk(i, carry):
        start = pl.multiple_of(i * 32, 32)
        normed[pl.ds(HALO + start, 32), :] = normalise(tokens[pl.ds(start, 32), :])
        return carry

    chunks = rows // 32
    early = chunks - 2 * PIECES if chunks > 2 * PIECES else 0
    lax.fori_loop(0, early, normalise_chunk, 0)

    def normalise_late(i, carry):
        for q in range(PIECES):

            @pl.when(i == q)
            def _():
                relay_piece(0, 1, q)

        each = (chunks - early) // PIECES
        return lax.fori_loop(early + i * each, early + (i + 1) * each, normalise_chunk, carry)

    lax.fori_loop(0, PIECES, normalise_late, 0)
    for d in range(2):
        halo_copy(d).wait_recv()
        normed[(0 if d == 0 else HALO + rows) : (HALO if d == 0 else 2 * HALO + rows), :] = (
            normalise(halo_in[d])
        )

    def slice_of(source):
        return normed[:, pl.ds(pl.multiple_of(source * shard, shard), shard)]

    def project(sources, tile, first):
        columns = slice(tile * TILE, (tile + 1) * TILE)
        term = functools.reduce(
            jnp.add, [dot(slice_of(o), win[o, :, columns]) for o in sources]
        )
        if first:
            acc[:, columns] = term
        else:
            acc[:, columns] += term

    for tile in range(WIN_COLS // TILE):
        project([me], tile, True)

    heads = lax.broadcasted_iota(jnp.int32, (LANES, step_w.shape[0]), 1)
    lanes_of = lax.broadcasted_iota(jnp.int32, (LANES, step_w.shape[0]), 0)
    spread = (heads == 2 * my_tp + lanes_of // (LANES // 2)).astype(BF16)
    step_cols[...] = dot(spread, step_w[...]).astype(BF16)
    tri = (
        lax.broadcasted_iota(jnp.int32, (BLOCK, BLOCK), 0)
        >= lax.broadcasted_iota(jnp.int32, (BLOCK, BLOCK), 1)
    ).astype(F32)
    first_head = half_lanes((1, LANES))
    first_rows = lax.broadcasted_iota(jnp.int32, (LANES, BLOCK), 0) < LANES // 2

    def decay_block(b):
        start = pl.multiple_of(b * BLOCK, BLOCK)
        raw = lax.dot_general(
            normed[pl.ds(HALO + start, BLOCK), :],
            step_cols[...],
            (((1,), (1,)), ((), ())),
            preferred_element_type=F32,
        )
        step = jnp.maximum(raw, 0.0) + jnp.log1p(jnp.exp(-jnp.abs(raw)))
        rate_row = jnp.where(first_head, rate[:, 0:1], rate[:, 1:2])
        jump = jumps[:, pl.ds(start, BLOCK)]
        logs = -rate_row * step + jnp.where(first_rows, jump[0:1, :], jump[1:2, :]).T
        step_b[pl.ds(start, BLOCK), :] = step
        cum_b[pl.ds(start, BLOCK), :] = dot(tri, logs, HIGHEST)

    angle_rows = rows // half

    def angle_block(i):
        start = pl.multiple_of(i * angle_rows, angle_rows)
        lane = lax.broadcasted_iota(jnp.int32, (angle_rows, LANES), 1)
        position = (
            lax.broadcasted_iota(jnp.int32, (angle_rows, LANES), 0) + me * rows + start
        )
        row_at = (position // GRID_WIDTH).astype(F32)
        col_at = lax.rem(position, GRID_WIDTH).astype(F32)
        exponent = lax.rem(lane, QUARTER).astype(F32) / -QUARTER
        inverse = jnp.exp(exponent[0:8] * 9.210340371976184)[0:1]
        angle = jnp.where(lane < LANES // 2, row_at, col_at) * inverse
        sine = jnp.sin(angle)
        cos_t[pl.ds(start, angle_rows), :] = jnp.cos(angle)
        sin_t[pl.ds(start, angle_rows), :] = jnp.where(
            lax.rem(lane, 2 * QUARTER) < QUARTER, -sine, sine
        )

    out_lag = OUT_LAG if half > OUT_LAG else 1

    def gather_step(s, carry):
        @pl.when(s == out_lag + 1)
        def _():
            set_off(1)

        before = s - 2
        for q in range(WIN_COLS // TILE):
            if q % 2 == 0:
                relay_piece(0, s, q // 2)
            else:
                relay_piece(1, s - 1 - out_lag, q // 2)
            if q == 0:
                y_landed(0, before)

            @pl.when((before >= 1) & (before < half))
            def _():
                project([origin(0, before), origin(1, before)], q, False)

            @pl.when(before == half)
            def _():
                project([origin(0, before)], q, False)

            if q == 1:

                @pl.when(s - 1 <= half)
                def _():
                    angle_block(s - 2)

            if q == 2:

                @pl.when(s - 1 <= blocks)
                def _():
                    decay_block(s - 2)

        return carry

    lax.fori_loop(2, half + 3, gather_step, 0)
    for b in range(half + 1, blocks):
        decay_block(b)

    def rotate(x, b):
        start = pl.multiple_of(b * BLOCK, BLOCK)
        wide = x.astype(BF16).astype(F32)
        lane = lax.broadcasted_iota(jnp.int32, (BLOCK, LANES), 1)
        turned = jnp.where(
            lax.rem(lane, 2 * QUARTER) < QUARTER,
            pltpu.roll(wide, LANES - QUARTER, 1),
            pltpu.roll(wide, QUARTER, 1),
        )
        return (
            wide * cos_t[pl.ds(start, BLOCK), :] + turned * sin_t[pl.ds(start, BLOCK), :]
        ).astype(BF16)

    def key_block(b, carry):
        start = pl.multiple_of(b * BLOCK, BLOCK)
        own = pl.ds(HALO + start, BLOCK)
        target = pl.ds(BLOCK + start, BLOCK)
        kv_ext[target, 0:LANES] = rotate(acc[own, 768:896], b)
        kv_ext[target, LANES : 2 * LANES] = acc[own, 896:1024].astype(BF16)
        return carry

    def query_block(b, carry):
        start = pl.multiple_of(b * BLOCK, BLOCK)
        own = pl.ds(HALO + start, BLOCK)
        for h in range(2):
            query_rot[pl.ds(start, BLOCK), h * LANES : (h + 1) * LANES] = rotate(
                acc[own, 512 + h * LANES : 512 + (h + 1) * LANES], b
            )
        return carry

    lax.fori_loop(0, blocks, key_block, 0)

    def kv_copy(d):
        source = kv_ext.at[pl.ds(rows if d == 0 else BLOCK, BLOCK)]
        return pltpu.make_async_remote_copy(
            source,
            kv_ext.at[pl.ds(0 if d == 0 else rows + BLOCK, BLOCK)],
            ks.at[d],
            kr.at[d],
            device_id={"sp": right if d == 0 else left},
        )

    pre[...] = acc[:, 0:384].astype(BF16).astype(F32)

    @pl.when(me == 0)
    def _():
        pre[0:HALO, :] = jnp.zeros((HALO, 384), F32)

    @pl.when(me == n - 1)
    def _():
        pre[HALO + rows : 2 * HALO + rows, :] = jnp.zeros((HALO, 384), F32)

    for d in range(2):
        kv_copy(d).start()

    taps = [f[...].astype(F32) for f in (filter_value, filter_keys, filter_query)]
    for b in range(blocks):
        for c in range(3):
            total = jnp.zeros((BLOCK, LANES), F32)
            for j in range(5):
                at = HALO + b * BLOCK + j - 2
                total = total + (
                    pre[at : at + BLOCK, c * LANES : (c + 1) * LANES] * taps[c][j : j + 1, :]
                )
            here = slice(b * BLOCK, (b + 1) * BLOCK)
            if c == 0:
                scan_v[here, :] = total * jax.nn.sigmoid(total) * step_b[here, :]
            elif c == 1:
                scan_k[here, :] = total.astype(BF16)
            else:
                scan_q[here, :] = total.astype(BF16)

    def block_states(b, carry):
        start = pl.multiple_of(b * BLOCK, BLOCK)
        here = pl.ds(start, BLOCK)
        cum = cum_b[here, :]
        total = cum[BLOCK - 1 : BLOCK, :]
        values = scan_v[here, :].astype(BF16).astype(F32)
        keys_t = scan_k[here, :].astype(F32).T.astype(BF16)
        state_a[b] = dot(keys_t, (values * jnp.exp(total - cum)).astype(BF16))
        state_c[b] = dot(keys_t, (values * jnp.exp(cum)).astype(BF16))
        return carry

    lax.fori_loop(0, blocks, block_states, 0)
    ends = [cum_b[(b + 1) * BLOCK - 1 : (b + 1) * BLOCK, :] for b in range(blocks)]
    forward = jnp.zeros((BLOCK, LANES), F32)
    for b in range(blocks):
        carry_f[b] = forward.astype(BF16)
        forward = forward * jnp.exp(ends[b]) + state_a[b]
    backward = jnp.zeros((BLOCK, LANES), F32)
    for b in reversed(range(blocks)):
        carry_b[b] = backward.astype(BF16)
        backward = backward * jnp.exp(ends[b]) + state_c[b]
    overall = functools.reduce(jnp.add, ends)

    piece = BLOCK // n
    message[...] = jnp.concatenate(
        [forward.reshape(n, piece, LANES), backward.reshape(n, piece, LANES)], axis=1
    ).astype(BF16)
    totals_out[...] = overall
    totals[me] = overall
    arrived[me] = message[me]

    def first_exchange(o):
        to = modulo(me + o, n)
        return (
            pltpu.make_async_remote_copy(
                message.at[to], arrived.at[me], a1s.at[o], a1r.at[o], device_id={"sp": to}
            ),
            pltpu.make_async_remote_copy(
                totals_out, totals.at[me], ts.at[o], tr.at[o], device_id={"sp": to}
            ),
        )

    def first_arrival(o):
        source = modulo(me - o, n)
        return (
            pltpu.make_async_remote_copy(
                arrived.at[source], arrived.at[source], a1s.at[o], a1r.at[o], device_id={"sp": source}
            ),
            pltpu.make_async_remote_copy(
                totals.at[source], totals.at[source], ts.at[o], tr.at[o], device_id={"sp": source}
            ),
        )

    order = sorted(range(1, n), key=lambda o: -min(o, n - o))
    for o in order:
        for copy in first_exchange(o):
            copy.start()

    out_next = [half + 2 - out_lag]

    def serve_out(last=False):
        while out_next[0] <= half:
            relay(1, out_next[0])
            out_next[0] += 1
            if not last:
                break

    serve_out()

    near_mask = half_lanes((BLOCK, LANES))

    def local_scan(b, carry):
        start = pl.multiple_of(b * BLOCK, BLOCK)
        here = pl.ds(start, BLOCK)
        cum = cum_b[here, :]
        cum_t = cum.T
        total = cum[BLOCK - 1 : BLOCK, :]
        values = scan_v[here, :].astype(BF16)
        query = scan_q[here, :]
        gram = lax.dot_general(
            query, scan_k[here, :], (((1,), (1,)), ((), ())), preferred_element_type=F32
        )
        near = []
        for h in range(2):
            lane = h * (LANES // 2)
            gap = jnp.abs(cum[:, lane : lane + 1] - cum_t[lane : lane + 1, :])
            near.append(dot((gram * jnp.exp(-gap)).astype(BF16), values))
        out = jnp.where(near_mask, near[0], near[1])
        out += jnp.exp(cum) * dot(query, carry_f[b])
        out += jnp.exp(total - cum) * dot(query, carry_b[b])
        scan_loc[here, :] = out
        return carry

    lax.fori_loop(0, blocks, local_scan, 0)

    lax.fori_loop(0, blocks, query_block, 0)
    for d in range(2):
        kv_copy(d).wait_recv()

    def attend(b, carry):
        start = pl.multiple_of(b * BLOCK, BLOCK)
        band = kv_ext[pl.ds(start, 3 * BLOCK), :]
        row = lax.broadcasted_iota(jnp.int32, (BLOCK, 3 * BLOCK), 0)
        col = lax.broadcasted_iota(jnp.int32, (BLOCK, 3 * BLOCK), 1)
        where_key = me * rows - BLOCK + start + col
        valid = (
            (jnp.abs(col - BLOCK - row) <= BLOCK) & (where_key >= 0) & (where_key < n * rows)
        )
        for h in range(2):
            query = query_rot[pl.ds(start, BLOCK), h * LANES : (h + 1) * LANES]
            scores = lax.dot_general(
                query, band[:, 0:LANES], (((1,), (1,)), ((), ())), preferred_element_type=F32
            ) * LANES ** (-0.5)
            masked = jnp.where(valid, scores, -1e30)
            ceiling = jnp.maximum(jnp.max(masked, axis=-1, keepdims=True), sink[:, h : h + 1])
            weights = jnp.where(valid, jnp.exp(masked - ceiling), 0.0)
            bottom = jnp.exp(sink[:, h : h + 1] - ceiling) + jnp.sum(weights, axis=-1, keepdims=True)
            probs = (weights / bottom).astype(BF16)
            mix[pl.ds(start, BLOCK), (1 + h) * LANES : (2 + h) * LANES] = dot(
                probs, band[:, LANES : 2 * LANES]
            ).astype(BF16)
        return carry

    lax.fori_loop(0, blocks // 2, attend, 0)
    serve_out()

    lax.fori_loop(blocks // 2, blocks, attend, 0)

    for o in order:
        for copy in first_arrival(o):
            copy.wait_recv()

    running = jnp.zeros((piece, LANES), F32)
    ahead = []
    for d in range(n):
        ahead.append(running)
        running = running * jnp.exp(totals[d]) + arrived[d].astype(F32)[0:piece]
    running = jnp.zeros((piece, LANES), F32)
    behind = [None] * n
    for d in reversed(range(n)):
        behind[d] = running
        running = running * jnp.exp(totals[d]) + arrived[d].astype(F32)[piece : 2 * piece]
    for d in range(n):
        income_out[d] = jnp.concatenate([ahead[d], behind[d]], axis=0).astype(BF16)
    incoming[me] = income_out[me]

    def second_exchange(o):
        to = modulo(me + o, n)
        return pltpu.make_async_remote_copy(
            income_out.at[to], incoming.at[me], a2s.at[o], a2r.at[o], device_id={"sp": to}
        )

    def second_arrival(o):
        source = modulo(me - o, n)
        return pltpu.make_async_remote_copy(
            incoming.at[source], incoming.at[source], a2s.at[o], a2r.at[o], device_id={"sp": source}
        )

    for o in order:
        second_exchange(o).start()

    serve_out(True)

    def wait_out(s, carry):
        y_landed(1, s)
        return carry

    lax.fori_loop(1, half + 1, wait_out, 0)

    def out_weights(i, low, size):
        return jnp.concatenate(
            [wout[2 * i, low : low + size, :], wout[2 * i + 1, low : low + size, :]], axis=1
        )

    spread_tiles = 4 if n % 8 == 0 else 1

    def window_product(i, carry):
        for u in range(spread_tiles):
            t = i * spread_tiles + u
            columns = pl.ds(pl.multiple_of(t * 2 * LANES, 2 * LANES), 2 * LANES)
            part_sum[:, columns] = dot(mix[:, LANES:], out_weights(t, LANES, 2 * LANES))
        return carry

    lax.fori_loop(0, n // 2 // spread_tiles, window_product, 0)

    for o in order:
        second_arrival(o).wait_recv()
    incomes = incoming[...].astype(F32)
    income_f = incomes[:, 0:piece].reshape(BLOCK, LANES).astype(BF16)
    income_b = incomes[:, piece : 2 * piece].reshape(BLOCK, LANES).astype(BF16)
    befores = [jnp.zeros((1, LANES), F32)]
    for b in range(blocks):
        befores.append(befores[-1] + ends[b])
    for b in range(blocks):
        here = slice(b * BLOCK, (b + 1) * BLOCK)
        cum = cum_b[here, :]
        query = scan_q[here, :]
        after = overall - befores[b + 1]
        out = scan_loc[here, :]
        out += jnp.exp(cum + befores[b]) * dot(query, income_f)
        out += jnp.exp(ends[b] - cum + after) * dot(query, income_b)
        gate = acc[HALO + b * BLOCK : HALO + (b + 1) * BLOCK, 384:512].astype(BF16).astype(F32)
        gated = out * (gate * jax.nn.sigmoid(gate))
        square = gated * gated
        low = jnp.sum(jnp.where(near_mask, square, 0.0), axis=-1, keepdims=True)
        high = jnp.sum(jnp.where(near_mask, 0.0, square), axis=-1, keepdims=True)
        mean = jnp.where(near_mask, low, high) * (2.0 / LANES)
        mix[here, 0:LANES] = (gated * lax.rsqrt(mean + 1e-06) * gain[...]).astype(BF16)

    unit = rows // (2 * nx)

    def group_product(x):
        first = pl.multiple_of(x * 2 * unit, 2 * unit)
        theirs = pl.multiple_of((1 - core) * unit, unit)
        lhs = mix[pl.ds(first, 2 * unit), 0:LANES]
        for t in range(n // 2):
            columns = slice(t * 2 * LANES, (t + 1) * 2 * LANES)
            part_sum[pl.ds(first, 2 * unit), columns] += dot(lhs, out_weights(t, 0, LANES))
        pair_out[x] = part_sum[pl.ds(first + theirs, unit), :].astype(BF16)

    def pair_copy(x):
        return pltpu.make_async_remote_copy(
            pair_out.at[x], pair_in.at[x], ps.at[x], pr.at[x], device_id={"tp": partner}
        )

    def group_step(i, carry):
        x = modulo(my_x + nx // 2 + i * (nx - 1), nx)
        group_product(x)
        pair_copy(x).start()
        return carry

    lax.fori_loop(0, nx, group_step, 0)

    side = unit // 2

    def group_sum(x, h):
        first = pl.multiple_of((2 * x + core) * unit + h * side, side)
        return part_sum[pl.ds(first, side), :] + pair_in[x, h * side : (h + 1) * side, :].astype(
            F32
        )

    next_x, last_x = modulo(my_x + 1, nx), modulo(my_x - 1, nx)

    def x_copy(i, source, target, d):
        return pltpu.make_async_remote_copy(
            source.at[d],
            target.at[d],
            gs.at[i, d],
            gr.at[i, d],
            device_id={"tp": 2 * (next_x if d == 0 else last_x) + core},
        )

    def via(d):
        return x_copy(0, via_out, via_in, d)

    def direct(d):
        return x_copy(1, direct_out, direct_in, d)

    def merged(d):
        return x_copy(2, merged_out, merged_in, d)

    beside = (next_x, last_x)

    if nx == 4:
        far = modulo(my_x + 2, nx)
        pair_copy(far).wait_recv()
        for d in range(2):
            via_out[d] = group_sum(far, d).astype(BF16)
            via(d).start()
    if nx > 1:
        for x in sorted({0, 1} if nx > 2 else {0}):
            pair_copy(beside[x]).wait_recv()
        for d in range(2):
            direct_out[d] = group_sum(beside[d], 1 - d).astype(BF16)
            direct(d).start()
    if nx == 4:
        for d in range(2):
            via(d).wait_recv()
            merged_out[d] = (group_sum(beside[d], d) + via_in[d].astype(F32)).astype(BF16)
            merged(d).start()
    pair_copy(my_x).wait_recv()
    for h in range(2):
        mine = group_sum(my_x, h)
        if nx > 1:
            direct(1 - h).wait_recv()
            mine = mine + direct_in[1 - h].astype(F32)
        if nx == 4:
            merged(h).wait_recv()
            mine = mine + merged_in[h].astype(F32)
        result[h * side : (h + 1) * side, :] = mine.astype(BF16)

    for d in range(2):
        halo_copy(d).wait_send()
        kv_copy(d).wait_send()
    for o in order:
        for copy in first_exchange(o):
            copy.wait_send()
        second_exchange(o).wait_send()
    for x in range(nx):
        pair_copy(x).wait_send()
    for d in range(2):
        if nx == 4:
            via(d).wait_send()
            merged(d).wait_send()
        if nx > 1:
            direct(d).wait_send()

    def drain(s, carry):
        def left(k, q, d):
            @pl.when(relays)
            def _():
                z_copy(d, s, k, q).wait_send()
                y_copy(d, s, k, q, own_half).wait_send()
                p_side(d, s, k, q).wait_send()
                p_down(d, s, k, q).wait_send()

                @pl.when(s > 1)
                def _():
                    p_copy(d, s, k, q).wait_send()

        for k in range(2):
            for q in range(pieces[k]):
                for d in range(2):
                    if last_way(k, q, d):
                        left(k, q, d)
                    else:

                        @pl.when(s < half)
                        def _():
                            left(k, q, d)

        return carry

    lax.fori_loop(1, half + 1, drain, 0)

    @pl.when(jnp.logical_not(relays))
    def _():
        for k in range(2):
            for d, q in first_pieces(k):
                p_first(d, k, q).wait_send()


def solution(mesh):
    n, ny, nt = (mesh.shape[a] for a in ("sp", "fs", "tp"))
    nx = nt // 2

    def shards(*args):
        args = list(args)
        rows, depth = args[0].shape
        for i in (1, 7, 9, 16):
            args[i] = args[i].reshape(1, -1)
        for i in (6, 8):
            args[i] = args[i].T
        shard = depth // n
        half = n // 2
        blocks = rows // BLOCK
        piece = BLOCK // n
        unit = rows // (2 * nx)
        vmem = pl.BlockSpec(memory_space=pltpu.VMEM)
        specs = [pl.BlockSpec(memory_space=pl.ANY)] * 19
        dma = pltpu.SemaphoreType.DMA
        V = pltpu.VMEM
        kept = (0, 1, 6, 7, 8, 9, 10, 11, 12, 16)
        scratch = [V(args[i].shape, args[i].dtype) for i in kept]
        scratch += [
            V((n, shard, WIN_COLS), BF16),
            V((n, 3 * LANES, LANES), BF16),
            V((n, shard // 2, WIN_COLS), BF16),
            V((n, 3 * LANES // 2, LANES), BF16),
            V((rows + 2 * HALO, depth), BF16),
            V((rows + 2 * HALO, WIN_COLS), F32),
            V((2, HALO, depth), BF16),
            V((rows + 2 * HALO, 3 * LANES), F32),
            V((rows, LANES), F32),
            V((rows, LANES), F32),
            V((rows, LANES), F32),
            V((rows, LANES), F32),
            V((LANES, depth), BF16),
            V((rows, LANES), F32),
            V((rows, LANES), BF16),
            V((rows, LANES), BF16),
            V((rows, 2 * LANES), BF16),
            V((rows + 2 * BLOCK, 2 * LANES), BF16),
            V((blocks, BLOCK, LANES), F32),
            V((blocks, BLOCK, LANES), F32),
            V((blocks, BLOCK, LANES), BF16),
            V((blocks, BLOCK, LANES), BF16),
            V((rows, LANES), F32),
            V((n, 2 * piece, LANES), BF16),
            V((n, 2 * piece, LANES), BF16),
            V((1, LANES), F32),
            V((n, 1, LANES), F32),
            V((n, 2 * piece, LANES), BF16),
            V((n, 2 * piece, LANES), BF16),
            V((rows, 3 * LANES), BF16),
            V((rows, depth), F32),
            V((nx, unit, depth), BF16),
            V((nx, unit, depth), BF16),
            *[V((2, unit // 2, depth), BF16)] * 6,
            dma((19,)),
            *[dma((2, half, PIECES))] * 4,
            *[dma((2, half, 2))] * 4,
            *[dma((2, half, PIECES))] * 5,
            *[dma((2, half, 2))] * 5,
            dma((2,)),
            dma((2,)),
            dma((2,)),
            dma((2,)),
            dma((n,)),
            dma((n,)),
            dma((n,)),
            dma((n,)),
            dma((n,)),
            dma((n,)),
            dma((nx,)),
            dma((nx,)),
            dma((3, 2)),
            dma((3, 2)),
        ]
        return pl.pallas_call(
            functools.partial(kernel, n, ny, nx),
            out_shape=jax.ShapeDtypeStruct((rows // nt, depth), BF16),
            in_specs=specs,
            out_specs=vmem,
            scratch_shapes=scratch,
            compiler_params=pltpu.CompilerParams(
                collective_id=0, has_side_effects=True, vmem_limit_bytes=60 * 1024 * 1024
            ),
        )(*args)

    placed = (
        P(("fs", "sp"), None),
        P(),
        P("sp", "tp"),
        P("sp", "tp"),
        P("sp", "tp"),
        P("sp", "tp"),
        P(),
        P("tp"),
        P(("fs", "sp"), "tp"),
        P("tp"),
        P(None, "tp"),
        P(None, "tp"),
        P(None, "tp"),
        P("sp", "tp"),
        P("sp", "tp"),
        P("sp", "tp"),
        P("tp"),
        P("tp", "sp"),
        P("tp", "sp"),
    )
    return jax.shard_map(
        shards, mesh=mesh, in_specs=placed, out_specs=P(("fs", "sp", "tp"), None), check_vma=False
    )
```
